32 devices in a mesh: sp: 8 (over z, y), tp: 4 (over x, core).
Axes of the slice: x: 2, y: 2, z: 4, core: 2. Of those that a mesh axis runs over, the one named last changes fastest.
Arguments:
- stream_in: bfloat16 [2048, 4096], P(('sp', 'tp')), may hold values from -6 to 6
- q_first: bfloat16 [2048, 1024], P('sp', 'tp'), may hold values from -110 to 110
- q_second: bfloat16 [2048, 1024], P('sp', 'tp'), may hold values from -110 to 110
- k_first: bfloat16 [2048, 512], P('sp', 'tp'), may hold values from -7 to 7
- k_second: bfloat16 [2048, 512], P('sp', 'tp'), may hold values from -7 to 7
- values: bfloat16 [2048, 1024], P('sp', 'tp'), may hold values from -6 to 6
- head_lambda: float32 [8], P('tp'), may hold values from 0.3 to 0.8
- w_out: bfloat16 [2048, 4096], P('tp'), may hold values from -0.125 to 0.125
- norm_gain: float32 [4096], replicated, may hold values from 0.1 to 1.9
- routes: int32 [2048, 4], P(('sp', 'tp')), may hold values from 0 to 7, all different within a row; in each aligned block of 64 rows (0 to 63, 64 to 127, ...) at most 48 rows name the same one
- route_w: float32 [2048, 4], P(('sp', 'tp')), may hold values from 0.2 to 1
- w_gate: bfloat16 [8, 4096, 128], P('sp'), may hold values from -0.09375 to 0.09375
- w_up: bfloat16 [8, 4096, 128], P('sp'), may hold values from -0.09375 to 0.09375
- w_down: bfloat16 [8, 128, 4096], P('sp'), may hold values from -0.5 to 0.5
- s_gate: bfloat16 [4096, 512], P(None, 'tp'), may hold values from -0.09375 to 0.09375
- s_up: bfloat16 [4096, 512], P(None, 'tp'), may hold values from -0.09375 to 0.09375
- s_down: bfloat16 [512, 4096], P('tp'), may hold values from -0.25 to 0.25
Outputs:
- layer_out: bfloat16 [2048, 4096], P(('sp', 'tp'))
The draws below stay inside these ranges and needn't reach their ends.
Inputs may be any that keep to these rules, and one draw needn't show every extreme that they name: `routes`: each row names 4 different experts. Within the rows of one device (aligned blocks of 64 rows) no expert is named more than 48 times, and in some blocks one expert is named exactly 48 times.
All inputs are finite; a program needn't handle non-finite values.
Results may differ from the reference program's by a relative error of at most 0.017.
Values may be sent and summed in bfloat16 or wider, within the bound.
No kernel may reach another device: no remote copies, remote signals or barrier semaphores. Data moves between devices by JAX's collectives and lax.ppermute only.
A program may use at most 128 MiB of HBM per device.

```python
import math
import jax
import jax.numpy as jnp
import numpy as np
from jax import lax

D = 4096
HEAD = 128
HEADS = 8
KV_HEADS = 4
VD = 256
F = 128
SF = 512
TOPK = 4
ROWS = 64
TOKENS = 2048
EXP = 8
CAP = 48
N_SP = 8
N_TP = 4


def key_table(key, which):
    raw = jnp.clip(jax.random.normal(jax.random.fold_in(key, 100 + which), (TOKENS, KV_HEADS * HEAD), jnp.float32), -4.5, 4.5) * 1.3
    return raw


def query_table(key, which):
    raw = jnp.clip(jax.random.normal(jax.random.fold_in(key, 300 + which), (TOKENS, HEADS * HEAD), jnp.float32), -4.5, 4.5) * 1.3
    return raw


def draw_q_first(key, part):
    return query_table(key, 1).astype(jnp.bfloat16)


def draw_q_second(key, part):
    return query_table(key, 2).astype(jnp.bfloat16)


def draw_k_first(key, part):
    return key_table(key, 1).astype(jnp.bfloat16)


def draw_k_second(key, part):
    return key_table(key, 2).astype(jnp.bfloat16)


def level_of(rng, shape, split, smallest, largest):
    factor_of = 1.0
    for axis_at, blocks in split:
        draws = jax.random.uniform(jax.random.fold_in(jax.random.fold_in(rng, 6), axis_at), (blocks,), jnp.float32, smallest / len(split), largest / len(split))
        factor_of = factor_of * jnp.repeat(jnp.exp(draws), shape[axis_at] // blocks).reshape((-1,) + (1,) * (len(shape) - 1 - axis_at))
    return factor_of


def routed_block(own_key, own, number, rows, amount, top, bound, lean):
    ranking = jax.random.permutation(own_key, amount)
    packed, common = shares(amount, rows * top, bound, lean, True), shares(amount, rows * top, bound, lean, False)
    places = jnp.arange(amount)

    def named(tallies, rotation):
        used = int((tallies > 0).sum())
        fixed = max(1, used // 4)
        shifted = fixed + (places - fixed + rotation * (used - fixed)) % max(1, amount - fixed)
        return jnp.zeros((amount,), jnp.int32).at[ranking[jnp.where(places < fixed, places, shifted)]].set(jnp.asarray(tallies, jnp.int32))

    tallies = jnp.where(number % 4 == 0, named(packed, number // 4), named(common, number - number // 4 - 1))
    mixed = jax.random.permutation(jax.random.fold_in(own, 3), amount)
    source_of, sink = mixed[0:amount // 2 * 2:2], mixed[1:amount // 2 * 2:2]
    margin = jnp.minimum(tallies[source_of] - 1, bound - tallies[sink]) // 2
    margin = jnp.where((source_of == ranking[0]) | (sink == ranking[0]) | (tallies[sink] == 0), 0, jnp.maximum(margin, 0))
    shifted = jax.random.randint(jax.random.fold_in(own, 4), (amount // 2,), 0, 1 << 20) % (margin + 1)
    tallies = tallies.at[source_of].add(-shifted).at[sink].add(shifted)
    labels = jnp.searchsorted(jnp.cumsum(tallies), jnp.arange(rows * top), side="right").astype(jnp.int32)
    grid = labels.reshape(top, rows).T
    grid = grid[jax.random.permutation(jax.random.fold_in(own, 1), rows)]
    rotation = jax.random.randint(jax.random.fold_in(own, 2), (rows, 1), 0, top)
    return jnp.take_along_axis(grid, (jnp.arange(top)[None, :] + rotation) % top, axis=1)


def shares(amount, total, limit, skew, full):
    loads = [(1 << 20) // math.isqrt(standing ** skew) + 1 for standing in range(1, amount + 1)]
    largest = limit if full else min(limit, max(-(-total // amount), total * loads[0] // sum(loads)))
    least = 1 if total - largest >= amount - 1 else 0
    holding, spare = [largest] + [least] * (amount - 1), total - largest - least * (amount - 1)
    while spare > 0:
        candidates = [i for i in range(1, amount) if holding[i] < largest] or [i for i in range(1, amount) if holding[i] < limit]
        mass, left = sum([loads[i] for i in candidates]), spare
        for i in candidates:
            addition = min(limit - holding[i], max(1, left * loads[i] // mass), spare)
            holding[i] = holding[i] + addition
            spare = spare - addition
    return np.array(holding)


def normal_values(key, extent, deviation, most, shards=(), held_as=jnp.bfloat16):
    loudness = level_of(key, extent, shards, -0.22, 0.18) if shards else 1.0
    drawn = jax.random.normal(key, extent, jnp.float32) * deviation * loudness
    return jnp.minimum(jnp.maximum(drawn, -most), most).astype(held_as)


def setup_inputs(seed: int = 0) -> dict:
    keys = jax.random.split(jax.random.key(seed), 18)
    stream_in = normal_values(keys[0], (TOKENS, D), 1.0, 6.0, ((0, 32),))
    q_first = draw_q_first(jax.random.fold_in(keys[17], 71), 0)
    q_second = draw_q_second(jax.random.fold_in(keys[17], 71), 0)
    k_first = draw_k_first(jax.random.fold_in(keys[17], 71), 0)
    k_second = draw_k_second(jax.random.fold_in(keys[17], 71), 0)
    values = normal_values(keys[5], (TOKENS, KV_HEADS * VD), 1.0, 6.0, ((0, 8), (1, 4)))
    head_lambda = jnp.clip(0.3 + 0.5 * jax.random.uniform(keys[6], (HEADS,), jnp.float32) ** level_of(keys[6], (HEADS,), ((0, 4),), -0.2, 0.2), 0.3, 0.8)
    w_out = normal_values(keys[7], (HEADS * VD, D), (HEADS * VD) ** -0.5, 0.125, ((0, 4),))
    norm_gain = jnp.clip(1.0 + 0.18 * jax.random.normal(keys[8], (D,), jnp.float32), 0.1, 1.9)
    routes_keys = jax.random.split(jax.random.fold_in(keys[9], 1), TOKENS // ROWS)
    routes_turns = jax.random.permutation(jax.random.fold_in(keys[9], 3), TOKENS // ROWS)
    routes = jax.vmap(lambda own, number: routed_block(jax.random.fold_in(keys[9], 2), own, number, ROWS, EXP, TOPK, CAP, 1))(routes_keys, routes_turns).reshape((TOKENS, TOPK))
    route_w = jnp.clip(0.2 + 0.8 * jax.random.uniform(keys[10], (TOKENS, TOPK), jnp.float32) ** level_of(keys[10], (TOKENS, TOPK), ((0, 32),), -0.2, 0.2), 0.2, 1.0)
    w_gate = normal_values(keys[11], (EXP, D, F), D ** -0.5, 0.09375, ((0, 8),))
    w_up = normal_values(keys[12], (EXP, D, F), D ** -0.5, 0.09375, ((0, 8),))
    w_down = normal_values(keys[13], (EXP, F, D), F ** -0.5, 0.5, ((0, 8),))
    s_gate = normal_values(keys[14], (D, SF), D ** -0.5, 0.09375, ((1, 4),))
    s_up = normal_values(keys[15], (D, SF), D ** -0.5, 0.09375, ((1, 4),))
    s_down = normal_values(keys[16], (SF, D), SF ** -0.5, 0.25, ((0, 4),))
    return {"stream_in": stream_in, "q_first": q_first, "q_second": q_second, "k_first": k_first, "k_second": k_second, "values": values, "head_lambda": head_lambda, "w_out": w_out, "norm_gain": norm_gain, "routes": routes, "route_w": route_w, "w_gate": w_gate, "w_up": w_up, "w_down": w_down, "s_gate": s_gate, "s_up": s_up, "s_down": s_down}


FLOOR = -1e+30

def absorb(state, first_q, second_q, first_k, second_k, value_rows, query_pos, key_pos):
    allowed = key_pos[None, :] <= query_pos[:, None]
    scale = first_q.shape[-1] ** (-0.5)
    result = []
    pairs = ((first_q, first_k), (second_q, second_k))
    for index in range(2):
        query_rows, key_rows = pairs[index]
        peak, total, accum = (state[3 * index], state[3 * index + 1], state[3 * index + 2])
        scores = jnp.dot(query_rows, key_rows.T, preferred_element_type=jnp.float32) * scale
        scores = jnp.where(allowed, scores, FLOOR)
        raised = jnp.maximum(peak, scores.max(-1))
        weights = jnp.where(allowed, jnp.exp(scores - raised[:, None]), 0.0)
        fade = jnp.exp(peak - raised)
        total = total * fade + weights.sum(-1)
        accum = accum * fade[:, None] + jnp.dot(weights.astype(jnp.bfloat16), value_rows, preferred_element_type=jnp.float32)
        result += [raised, total, accum]
    return tuple(result)

def one_head(first_q, second_q, first_k, second_k, value_rows, weight, span, blocks):

    def per_block(block):
        begin = block * span
        query_one = lax.dynamic_slice_in_dim(first_q, begin, span, 0)
        query_two = lax.dynamic_slice_in_dim(second_q, begin, span, 0)
        query_pos = begin + jnp.arange(span, dtype=jnp.int32)
        peaks = jnp.full((span,), FLOOR, jnp.float32)
        sums = jnp.zeros((span,), jnp.float32)
        accums = jnp.zeros((span, VD), jnp.float32)
        start_state = (peaks, sums, accums, peaks, sums, accums)

        def visit(inner, state):
            key_begin = inner * span
            key_one = lax.dynamic_slice_in_dim(first_k, key_begin, span, 0)
            key_two = lax.dynamic_slice_in_dim(second_k, key_begin, span, 0)
            value_part = lax.dynamic_slice_in_dim(value_rows, key_begin, span, 0)
            key_pos = key_begin + jnp.arange(span, dtype=jnp.int32)
            return absorb(state, query_one, query_two, key_one, key_two, value_part, query_pos, key_pos)
        final = lax.fori_loop(jnp.int32(0), block + 1, visit, start_state)
        head_out = final[2] / final[1][:, None] - weight * final[5] / final[4][:, None]
        head_out = head_out * lax.rsqrt(lax.optimization_barrier(jnp.mean(head_out * head_out, axis=-1, keepdims=True)) + 1e-05)
        return head_out.astype(jnp.bfloat16)
    outputs = lax.map(per_block, jnp.arange(blocks, dtype=jnp.int32))
    return outputs.reshape(TOKENS, VD)

def reference(stream_in, q_first, q_second, k_first, k_second, values, head_lambda, w_out, norm_gain, routes, route_w, w_gate, w_up, w_down, s_gate, s_up, s_down):
    group = HEADS // KV_HEADS
    span = math.gcd(TOKENS, 512)
    blocks = TOKENS // span
    parts = []
    for head in range(HEADS):
        key_head = head // group
        parts.append(one_head(q_first[:, head * HEAD:(head + 1) * HEAD], q_second[:, head * HEAD:(head + 1) * HEAD], k_first[:, key_head * HEAD:(key_head + 1) * HEAD], k_second[:, key_head * HEAD:(key_head + 1) * HEAD], values[:, key_head * VD:(key_head + 1) * VD], head_lambda[head], span, blocks))
    attn_rows = jnp.concatenate(parts, axis=1)
    attn = jnp.dot(attn_rows, w_out, preferred_element_type=jnp.float32)
    resid = (stream_in.astype(jnp.float32) + attn).astype(jnp.bfloat16)
    stream = lax.optimization_barrier(resid).astype(jnp.float32)
    normed = (stream * lax.rsqrt(lax.optimization_barrier(jnp.mean(stream * stream, axis=-1, keepdims=True)) + 1e-06) * norm_gain).astype(jnp.bfloat16)
    shared_hidden = (jax.nn.silu(jnp.dot(normed, s_gate, preferred_element_type=jnp.float32)) * jnp.dot(normed, s_up, preferred_element_type=jnp.float32)).astype(jnp.bfloat16)
    shared = jnp.dot(shared_hidden, s_down, preferred_element_type=jnp.float32)
    flat_ids = routes.reshape(-1).astype(jnp.int32)
    count_all = TOKENS * TOPK
    token_of = jnp.arange(count_all, dtype=jnp.int32) // TOPK
    order = jnp.argsort(flat_ids, stable=True).astype(jnp.int32)
    counts = lax.optimization_barrier(jnp.sum((flat_ids[None, :] == jnp.arange(EXP, dtype=jnp.int32)[:, None]).astype(jnp.int32), axis=1)).astype(jnp.int32)
    starts = (jnp.cumsum(counts) - counts).astype(jnp.int32)
    window = N_SP * N_TP * CAP
    padded = jnp.concatenate([order, jnp.zeros((window,), jnp.int32)])
    flat_weights = route_w.reshape(-1)

    def serve(routed, inputs):
        gate_e, up_e, down_e, begin, count = inputs
        picks = lax.dynamic_slice_in_dim(padded, begin, window, 0)
        live = jnp.arange(window, dtype=jnp.int32) < count
        tokens_here = token_of[picks]
        rows_here = normed[tokens_here]
        hidden = (jax.nn.silu(jnp.dot(rows_here, gate_e, preferred_element_type=jnp.float32)) * jnp.dot(rows_here, up_e, preferred_element_type=jnp.float32)).astype(jnp.bfloat16)
        result = jnp.dot(hidden, down_e, preferred_element_type=jnp.float32).astype(jnp.bfloat16)
        scaled = result.astype(jnp.float32) * jnp.where(live, flat_weights[picks], 0.0)[:, None]
        return (routed.at[tokens_here].add(scaled), None)
    routed, _ = lax.scan(serve, jnp.zeros((TOKENS, D), jnp.float32), (w_gate, w_up, w_down, starts, counts))
    return (stream + routed + shared).astype(jnp.bfloat16)
```

```python
import math

import jax
import jax.numpy as jnp
from jax import lax
from jax.experimental import pallas as pl
from jax.experimental.pallas import tpu as pltpu
from jax.sharding import PartitionSpec as P

HEAD = 128
TURNS = (0, 2, 1, 3)


FLOOR = -1e30


def absorb(state, first_q, second_q, first_k, second_k, value_rows, query_pos, key_pos):
    allowed = key_pos[None, :] <= query_pos[:, None]
    scale = first_q.shape[-1] ** (-0.5)
    result = []
    pairs = ((first_q, first_k), (second_q, second_k))
    for index in range(2):
        query_rows, key_rows = pairs[index]
        peak, total, accum = (state[3 * index], state[3 * index + 1], state[3 * index + 2])
        scores = (
            jnp.einsum("qagd,kad->agqk", query_rows, key_rows, preferred_element_type=jnp.float32)
            * scale
        )
        scores = jnp.where(allowed, scores, FLOOR)
        raised = jnp.maximum(peak, scores.max(-1))
        weights = jnp.where(allowed, jnp.exp(scores - raised[..., None]), 0.0)
        fade = jnp.exp(peak - raised)
        total = total * fade + weights.sum(-1)
        accum = accum * fade[..., None] + jnp.einsum(
            "agqk,kad->agqd",
            weights.astype(jnp.bfloat16),
            value_rows,
            preferred_element_type=jnp.float32,
        )
        result += [raised, total, accum]
    return tuple(result)


def empty_state(kv_local, group, count, value_dim):
    peaks = jnp.full((kv_local, group, count), FLOOR, jnp.float32)
    sums = jnp.zeros((kv_local, group, count), jnp.float32)
    accums = jnp.zeros((kv_local, group, count, value_dim), jnp.float32)
    return (peaks, sums, accums, peaks, sums, accums)


def fold_rows(state, first_q, second_q, query_pos, last_row, pieces, start):
    first_k, second_k, value_rows = pieces
    length = first_k.shape[0]
    kv_local = first_q.shape[1]
    value_dim = value_rows.shape[1] // kv_local
    span = math.gcd(length, 2048)

    def sweep(current):

        def visit(block, inner):
            begin = block * span
            key_one = lax.dynamic_slice_in_dim(first_k, begin, span, 0).reshape(
                span, kv_local, HEAD
            )
            key_two = lax.dynamic_slice_in_dim(second_k, begin, span, 0).reshape(
                span, kv_local, HEAD
            )
            value_part = lax.dynamic_slice_in_dim(value_rows, begin, span, 0).reshape(
                span, kv_local, value_dim
            )
            key_pos = begin + jnp.arange(span, dtype=jnp.int32)
            return absorb(
                inner, first_q, second_q, key_one, key_two, value_part, query_pos, key_pos
            )

        return lax.fori_loop(0, length // span, visit, current)

    def unchanged(current):
        return current

    return lax.cond(start <= last_row, sweep, unchanged, state)


def finish_heads(final, head_lambda):
    kv_local, group, count, value_dim = final[2].shape
    weight = head_lambda.reshape(kv_local, group, 1, 1)
    head_out = final[2] / final[1][..., None] - weight * final[5] / final[4][..., None]
    head_out = head_out * lax.rsqrt(jnp.mean(head_out * head_out, axis=-1, keepdims=True) + 1e-05)
    return (
        head_out.transpose(2, 0, 1, 3)
        .reshape(count, kv_local * group * value_dim)
        .astype(jnp.bfloat16)
    )


def shared_part(normed, s_gate, s_up, s_down):
    piece = lax.all_gather(normed, "tp", axis=0, tiled=True)
    gate_part = jnp.dot(piece, s_gate, preferred_element_type=jnp.float32)
    up_part = jnp.dot(piece, s_up, preferred_element_type=jnp.float32)
    hidden = (jax.nn.silu(gate_part) * up_part).astype(jnp.bfloat16)
    terms = jnp.dot(hidden, s_down, preferred_element_type=jnp.float32)
    return lax.psum_scatter(
        terms.astype(jnp.bfloat16), "tp", scatter_dimension=0, tiled=True
    ).astype(jnp.float32)


def routed_part(normed, routes, route_w, w_gate, w_up, w_down):
    rows, topk = routes.shape
    local_experts = w_gate.shape[0]
    experts = local_experts * lax.axis_size("sp")
    slots = max(2, 3 * rows * topk // (2 * experts))
    flat_ids = routes.reshape(-1)
    hits = (flat_ids[:, None] == jnp.arange(experts, dtype=jnp.int32)[None, :]).astype(jnp.int32)
    slot_of = jnp.sum(jnp.cumsum(hits, axis=0) * hits, axis=1) - 1
    target = flat_ids * slots + slot_of
    placing = jnp.any(
        jnp.arange(experts * slots, dtype=jnp.int32)[:, None, None]
        == target.reshape(rows, topk)[None, :, :],
        axis=-1,
    ).astype(jnp.bfloat16)
    outgoing = (
        jnp.dot(placing, normed, preferred_element_type=jnp.float32)
        .astype(jnp.bfloat16)
        .reshape(experts, slots, normed.shape[1])
    )
    arrived = lax.all_to_all(outgoing, "sp", split_axis=0, concat_axis=0, tiled=True)
    sources = arrived.shape[0] // local_experts
    grouped = arrived.reshape(sources, local_experts, arrived.shape[1], arrived.shape[2])
    gate_part = jnp.einsum("sjcd,jdf->sjcf", grouped, w_gate, preferred_element_type=jnp.float32)
    up_part = jnp.einsum("sjcd,jdf->sjcf", grouped, w_up, preferred_element_type=jnp.float32)
    hidden = (jax.nn.silu(gate_part) * up_part).astype(jnp.bfloat16)
    result = jnp.einsum(
        "sjcf,jfd->sjcd", hidden, w_down, preferred_element_type=jnp.float32
    ).astype(jnp.bfloat16)
    returned = lax.all_to_all(
        result.reshape(arrived.shape), "sp", split_axis=0, concat_axis=0, tiled=True
    )
    picked = (
        returned.reshape(experts * slots, normed.shape[1])[target]
        .reshape(rows, topk, normed.shape[1])
        .astype(jnp.float32)
    )
    return jnp.sum(picked * route_w[..., None], axis=1)


def slow_local(
    stream_in,
    q_first,
    q_second,
    k_first,
    k_second,
    values,
    head_lambda,
    w_out,
    norm_gain,
    routes,
    route_w,
    w_gate,
    w_up,
    w_down,
    s_gate,
    s_up,
    s_down,
):
    seq_rows = q_first.shape[0]
    kv_local = k_first.shape[1] // HEAD
    heads_local = q_first.shape[1] // HEAD
    group = heads_local // kv_local
    value_dim = values.shape[1] // kv_local
    offset = lax.axis_index("sp") * seq_rows
    query_pos = offset + jnp.arange(seq_rows, dtype=jnp.int32)
    last_row = offset + seq_rows - 1
    first_q = q_first.reshape(seq_rows, kv_local, group, HEAD)
    second_q = q_second.reshape(seq_rows, kv_local, group, HEAD)
    start_state = empty_state(kv_local, group, seq_rows, value_dim)
    folded_state = fold_rows(
        start_state,
        first_q,
        second_q,
        query_pos,
        last_row,
        (
            lax.all_gather(k_first, "sp", axis=0, tiled=True),
            lax.all_gather(k_second, "sp", axis=0, tiled=True),
            lax.all_gather(values, "sp", axis=0, tiled=True),
        ),
        jnp.int32(0),
    )
    attn_rows = finish_heads(folded_state, head_lambda)
    attn = lax.psum_scatter(
        jnp.dot(attn_rows, w_out, preferred_element_type=jnp.float32).astype(jnp.bfloat16),
        "tp",
        scatter_dimension=0,
        tiled=True,
    ).astype(jnp.float32)
    resid = (stream_in.astype(jnp.float32) + attn).astype(jnp.bfloat16)
    stream = lax.optimization_barrier(resid).astype(jnp.float32)
    normed = (
        stream * lax.rsqrt(jnp.mean(stream * stream, axis=-1, keepdims=True) + 1e-06) * norm_gain
    ).astype(jnp.bfloat16)
    routed = routed_part(normed, routes, route_w, w_gate, w_up, w_down)
    shared = shared_part(normed, s_gate, s_up, s_down)
    return (stream + routed + shared).astype(jnp.bfloat16)


VMEM = pltpu.MemorySpace.VMEM
MIB = 1024 * 1024
SMEM = pltpu.MemorySpace.SMEM
HBM = pltpu.MemorySpace.HBM


def ring_order(count):
    return list(range(0, count, 2)) + list(range(count - 1, 0, -2))


def ring_pairs(count):
    order = ring_order(count)
    forward = [(order[i], order[(i + 1) % count]) for i in range(count)]
    return forward, [(b, a) for a, b in forward]


def ring_sources(count):
    order = ring_order(count)
    rows = [None] * count
    for place, index in enumerate(order):
        row = [index]
        for step in range(1, count // 2):
            row += [order[(place - step) % count], order[(place + step) % count]]
        row.append(order[(place + count // 2) % count])
        rows[index] = row
    return rows


def dot_nt(a, b):
    return lax.dot_general(a, b, (((1,), (1,)), ((), ())), preferred_element_type=jnp.float32)


def grouped(copies):
    for copy in copies:
        copy.start()
    return copies


def attn_kernel(spans, first, last, scale, own_rows, *refs):
    refs = list(refs)
    ids_ref = refs.pop(0)
    if last:
        lam_ref = refs.pop(0)
    q_in = [refs.pop(0), refs.pop(0)]
    kv_in = [refs.pop(0) for _ in spans]
    if not first:
        state_in = [refs.pop(0) for _ in range(3)]
    if last:
        w_ref, stream_ref = refs.pop(0), refs.pop(0)
        own_ref, send_ref, m_ref, l_ref, acc_ref, mixed_ref, w, stream, w_sem = refs[:9]
        del refs[:9]
        load = pltpu.make_async_copy(w_ref, w, w_sem.at[0])
        feed = pltpu.make_async_copy(stream_ref, stream, w_sem.at[1])
    elif first:
        q_refs = [refs.pop(0), refs.pop(0)]
        m_ref, l_ref, acc_ref = refs.pop(0), refs.pop(0), refs.pop(0)
    else:
        m_ref, l_ref, acc_ref = refs.pop(0), refs.pop(0), refs.pop(0)
    kv_scratch, sem = refs
    rows = q_in[0].shape[0]
    heads = q_in[0].shape[1] // HEAD
    parts = rows // own_rows
    me, mine = ids_ref[0], ids_ref[1]
    outs = (m_ref, l_ref, acc_ref)
    starts = [sum(b.shape[0] for b in kv_in[:at]) for at in range(len(spans))]
    kv_refs = [
        kv_scratch.at[pl.ds(start, ref.shape[0])] for start, ref in zip(starts, kv_in)
    ]
    copies = grouped(
        [
            pltpu.make_async_copy(source, into, sem.at[at])
            for at, (source, into) in enumerate(zip(kv_in, kv_refs))
        ]
    )
    if last:
        load.start()
        feed.start()
    if first:
        loads = grouped(
            [
                pltpu.make_async_copy(
                    q_in[which].at[
                        pl.ds(pl.multiple_of((mine ^ turn) * own_rows, own_rows), own_rows)
                    ],
                    q_refs[which].at[pl.ds(index * own_rows, own_rows)],
                    sem.at[len(spans) + which * parts + index],
                )
                for which in range(2)
                for index, turn in enumerate(TURNS)
            ]
        )
        for copy in loads:
            copy.wait()
    else:
        q_refs = q_in

    def fold(kv_ref, diagonal, old_refs=outs):
        keys = kv_ref.shape[0]
        v = kv_ref[:, 2 * HEAD :]
        old_m, old_l, old_acc = old_refs
        if diagonal:
            row_at = lax.broadcasted_iota(jnp.int32, (rows, keys), 0)
            key_at = lax.broadcasted_iota(jnp.int32, (rows, keys), 1)
            part = row_at // own_rows
            place = jnp.zeros_like(part)
            for index, turn in enumerate(TURNS):
                place = jnp.where(part == index, mine ^ turn, place)
            allowed = key_at <= place * own_rows + row_at % own_rows
        for head in range(heads):
            for which in range(2):
                pair = 2 * head + which
                q = q_refs[which][:, head * HEAD : (head + 1) * HEAD]
                k = kv_ref[:, which * HEAD : (which + 1) * HEAD]
                s = dot_nt(q, k)
                if diagonal:
                    s = jnp.where(allowed, s, FLOOR)
                top = jnp.max(s, axis=1, keepdims=True)
                if diagonal:
                    raised = jnp.broadcast_to(top, (rows, 128))
                else:
                    old = old_m[pair]
                    raised = jnp.maximum(old, top)
                wide = jnp.concatenate([raised] * (keys // 128), axis=1)
                p = jnp.exp((s - wide) * scale)
                part_sum = p[:, :128]
                for at in range(128, keys, 128):
                    part_sum = part_sum + p[:, at : at + 128]
                prod = jnp.dot(p.astype(jnp.bfloat16), v, preferred_element_type=jnp.float32)
                m_ref[pair] = raised
                if diagonal:
                    l_ref[pair] = part_sum
                    acc_ref[pair] = prod
                else:
                    fade = jnp.exp((old - raised) * scale)
                    l_ref[pair] = old_l[pair] * fade + part_sum
                    fades = jnp.concatenate([fade] * (prod.shape[1] // 128), axis=1)
                    acc_ref[pair] = old_acc[pair] * fades + prod

    for index, (place, pieces) in enumerate(spans):
        copies[index].wait()
        if pieces == 2:
            copies[index + 1].wait()
            kv_ref = kv_scratch.at[
                pl.ds(starts[index], kv_in[index].shape[0] + kv_in[index + 1].shape[0])
            ]
        elif pieces == 0:
            continue
        else:
            kv_ref = kv_refs[index]
        if first and index == 0:
            fold(kv_ref, True)
            continue
        earlier = ids_ref[2 + place] < me
        carry = not first and index == 0

        @pl.when(earlier)
        def _(kv_ref=kv_ref, carry=carry):
            fold(kv_ref, False, state_in if carry else outs)

        if carry:

            @pl.when(jnp.logical_not(earlier))
            def _():
                for into, source in zip(outs, state_in):
                    into[...] = source[...]

        if pieces == 2:
            break

    if last:
        for head in range(heads):
            terms = []
            for which in range(2):
                pair = 2 * head + which
                total = jnp.sum(l_ref[pair], axis=1, keepdims=True)
                terms.append(acc_ref[pair] / total)
            mixed = terms[0] - lam_ref[head] * terms[1]
            square = jnp.mean(mixed * mixed, axis=1, keepdims=True)
            mixed = mixed * lax.rsqrt(square + 1e-05)
            width = mixed.shape[1]
            mixed_ref[:, head * width : (head + 1) * width] = mixed.astype(jnp.bfloat16)
        load.wait()
        feed.wait()
        half = rows // 2
        step = math.gcd(w.shape[1], 512)

        def body(at, _):
            cols = pl.ds(pl.multiple_of(at * step, step), step)
            out = jnp.dot(mixed_ref[...], w[:, cols], preferred_element_type=jnp.float32)
            own_ref[:own_rows, cols] = out[:own_rows] + stream[:, cols].astype(jnp.float32)
            own_ref[own_rows:, cols] = out[own_rows:half]
            send_ref[:, cols] = out[half:].astype(jnp.bfloat16)
            return 0

        lax.fori_loop(0, w.shape[1] // step, body, 0)


def specs(space, count):
    return [pl.BlockSpec(memory_space=space)] * count


def attn_call(ids, q_first, q_second, blocks, spans, state, own_rows, lam=None, w_out=None, stream_in=None):
    rows = q_first.shape[0]
    heads = q_first.shape[1] // HEAD
    value_dim = blocks[0].shape[1] - 2 * HEAD
    first, last = state is None, w_out is not None
    states = [
        pltpu.VMEM((2 * heads, rows, 128), jnp.float32),
        pltpu.VMEM((2 * heads, rows, 128), jnp.float32),
        pltpu.VMEM((2 * heads, rows, value_dim), jnp.float32),
    ]
    operands = [ids] + ([lam] if last else []) + [q_first, q_second, *blocks]
    in_specs = specs(SMEM, 2 if last else 1)
    in_specs += specs(HBM if first else VMEM, 2) + specs(HBM, len(blocks))
    if not first:
        operands += list(state)
        in_specs += specs(VMEM, 3)
    scratch = []
    if last:
        operands += [w_out, stream_in]
        in_specs += specs(HBM, 2)
        width = w_out.shape[1]
        out_shape = [
            pltpu.VMEM((rows // 2, width), jnp.float32),
            jax.ShapeDtypeStruct((rows // 2, width), jnp.bfloat16),
        ]
        scratch = [
            *states,
            pltpu.VMEM((rows, heads * value_dim), jnp.bfloat16),
            pltpu.VMEM(w_out.shape, jnp.bfloat16),
            pltpu.VMEM(stream_in.shape, jnp.bfloat16),
            pltpu.SemaphoreType.DMA((2,)),
        ]
    else:
        out_shape = list(states)
        if first:
            out_shape = [pltpu.VMEM(q_first.shape, q_first.dtype)] * 2 + out_shape
    keys = sum(b.shape[0] for b in blocks)
    scratch += [
        pltpu.VMEM((keys, blocks[0].shape[1]), jnp.bfloat16),
        pltpu.SemaphoreType.DMA((len(blocks) + 2 * rows // own_rows,)),
    ]
    body = lambda *refs: attn_kernel(spans, first, last, HEAD**-0.5, own_rows, *refs)
    return pl.pallas_call(
        body,
        out_shape=out_shape,
        in_specs=in_specs,
        out_specs=specs(VMEM, len(out_shape)),
        scratch_shapes=scratch,
        cost_estimate=pl.CostEstimate(
            flops=8 * heads * rows * keys * (HEAD + value_dim),
            bytes_accessed=4 * 1024 * 1024,
            transcendentals=2 * heads * rows * keys,
        ),
        compiler_params=pltpu.CompilerParams(vmem_limit_bytes=(22 if last else 12) * MIB),
    )(*operands)


def pack_kernel(one_ref, two_ref, three_ref, out_ref, sem):
    wide = one_ref.shape[1]
    cuts = ((0, wide), (wide, wide), (2 * wide, three_ref.shape[1]))
    copies = grouped(
        [
            pltpu.make_async_copy(ref, out_ref.at[:, pl.ds(start, size)], sem.at[at])
            for at, (ref, (start, size)) in enumerate(zip((one_ref, two_ref, three_ref), cuts))
        ]
    )
    for copy in copies:
        copy.wait()


def pack_call(one, two, three):
    width = one.shape[1] + two.shape[1] + three.shape[1]
    return pl.pallas_call(
        pack_kernel,
        out_shape=jax.ShapeDtypeStruct((one.shape[0], width), one.dtype),
        in_specs=specs(HBM, 3),
        out_specs=pl.BlockSpec(memory_space=VMEM),
        scratch_shapes=[pltpu.SemaphoreType.DMA((3,))],
        name="pack",
    )(one, two, three)


def slices_kernel(unit, ids_ref, gate_ref, up_ref, down_ref, gate_out, rest_out, gate, up, turned, sem):
    start = pl.multiple_of(ids_ref[1] * unit, unit)
    loads = grouped(
        [
            pltpu.make_async_copy(gate_ref, gate, sem.at[0]),
            pltpu.make_async_copy(up_ref, up, sem.at[1]),
            pltpu.make_async_copy(
                down_ref.at[pl.ds(start, unit)], rest_out.at[pl.ds(unit, unit)], sem.at[2]
            ),
        ]
    )
    loads[0].wait()
    turned[...] = gate[...].T
    gate_out[...] = turned[pl.ds(start, unit)]
    loads[1].wait()
    turned[...] = up[...].T
    rest_out[:unit] = turned[pl.ds(start, unit)]
    loads[2].wait()


def slices_call(ids, gate, up, down, unit):
    width = gate.shape[0]
    return pl.pallas_call(
        lambda *refs: slices_kernel(unit, *refs),
        out_shape=[
            jax.ShapeDtypeStruct((unit, width), gate.dtype),
            jax.ShapeDtypeStruct((2 * unit, width), gate.dtype),
        ],
        in_specs=specs(SMEM, 1) + specs(HBM, 3),
        out_specs=specs(VMEM, 2),
        scratch_shapes=[
            pltpu.VMEM(gate.shape, gate.dtype),
            pltpu.VMEM(up.shape, gate.dtype),
            pltpu.VMEM((gate.shape[1], width), gate.dtype),
            pltpu.SemaphoreType.DMA((3,)),
        ],
        name="slices",
    )(ids, gate, up, down)


def silu(v):
    return v / (1.0 + jnp.exp(-v))


def stack_kernel(unit, gates_count, rests_count, *refs):
    refs = list(refs)
    gates = [refs.pop(0) for _ in range(gates_count)]
    rests = [refs.pop(0) for _ in range(rests_count)]
    sg_ref, su_ref, sd_ref, gate_out, up_out, down_out, sg_out, su_out, sem = refs
    moves = [(sg_ref, sg_out), (su_ref, su_out)]
    at = 0
    for ref in gates:
        moves.append((ref, gate_out.at[pl.ds(at, ref.shape[0])]))
        at += ref.shape[0]
    for index, ref in enumerate(rests):
        moves.append((ref.at[pl.ds(0, unit)], up_out.at[pl.ds(index * unit, unit)]))
        moves.append((ref.at[pl.ds(unit, unit)], down_out.at[pl.ds(index * unit, unit)]))
    moves.append((sd_ref, down_out.at[pl.ds(rests_count * unit, sd_ref.shape[0])]))
    copies = grouped(
        [pltpu.make_async_copy(a, b, sem.at[k]) for k, (a, b) in enumerate(moves)]
    )
    for copy in copies:
        copy.wait()


def stack_call(gates, rests, s_gate, s_up, s_down):
    unit = rests[0].shape[0] // 2
    width = rests[0].shape[1]
    operands = [*gates, *rests, s_gate, s_up, s_down]
    total = sum(g.shape[0] for g in gates)
    most = len(rests) * unit
    return pl.pallas_call(
        lambda *refs: stack_kernel(unit, len(gates), len(rests), *refs),
        out_shape=[
            pltpu.VMEM((total, width), jnp.bfloat16),
            pltpu.VMEM((most, width), jnp.bfloat16),
            pltpu.VMEM((most + s_down.shape[0], width), jnp.bfloat16),
            pltpu.VMEM(s_gate.shape, jnp.bfloat16),
            pltpu.VMEM(s_up.shape, jnp.bfloat16),
        ],
        in_specs=specs(HBM, len(operands)),
        out_specs=specs(VMEM, 5),
        scratch_shapes=[pltpu.SemaphoreType.DMA((len(gates) + 2 * len(rests) + 3,))],
        cost_estimate=pl.CostEstimate(flops=10**9, bytes_accessed=16 * MIB, transcendentals=0),
        compiler_params=pltpu.CompilerParams(vmem_limit_bytes=2 * MIB),
        name="stack",
    )(*operands)


def spread(ids_ref, combine, first, count, unit):
    expert = lax.broadcasted_iota(jnp.int32, combine.shape, 1)
    columns = []
    for block in range(first, first + count):
        picked = jnp.where(expert == ids_ref[2 + block], combine, 0.0)
        column = jnp.sum(picked, axis=1, keepdims=True)
        columns.append(jnp.broadcast_to(column, (combine.shape[0], unit)))
    return jnp.concatenate(columns, axis=1)


def most_kernel(count, unit, ids_ref, one_ref, two_ref, near_ref, far_ref, *refs):
    refs = list(refs)
    late = [refs.pop(0) for _ in range(count)]
    gate_ref, up_ref, down_ref, sg_ref, su_ref, out_ref, x_ref, late_ref, hidden_ref, sem = refs
    half = one_ref.shape[0]
    moves = [(one_ref, x_ref.at[pl.ds(0, half)]), (two_ref, x_ref.at[pl.ds(half, half)])]
    moves += [
        (ref, late_ref.at[pl.ds(2 * unit * index, 2 * unit)]) for index, ref in enumerate(late)
    ]
    copies = grouped(
        [pltpu.make_async_copy(a, b, sem.at[k]) for k, (a, b) in enumerate(moves)]
    )
    copies[0].wait()
    copies[1].wait()
    x = x_ref[...]
    begun = up_ref.shape[0]
    used = begun + count * unit
    gate = dot_nt(x, gate_ref[:used])
    for copy in copies[2:]:
        copy.wait()
    ups = [late_ref[2 * unit * index : 2 * unit * index + unit] for index in range(count)]
    up = dot_nt(x, jnp.concatenate([up_ref[...]] + ups, axis=0))
    combine = jnp.concatenate([near_ref[...], far_ref[...]], axis=0)
    scale = spread(ids_ref, combine, 0, used // unit, unit)
    hidden = (silu(gate) * up * scale).astype(jnp.bfloat16)
    gate = jnp.dot(x, sg_ref[...], preferred_element_type=jnp.float32)
    up = jnp.dot(x, su_ref[...], preferred_element_type=jnp.float32)
    shared = (silu(gate) * up).astype(jnp.bfloat16)
    hidden_ref[:, :begun] = hidden[:, :begun]
    hidden_ref[:, begun : begun + shared.shape[1]] = shared
    hidden_ref[:, begun + shared.shape[1] :] = hidden[:, begun:]
    width = out_ref.shape[1]
    step = math.gcd(width, 512)

    def body(at, _):
        cols = pl.ds(pl.multiple_of(at * step, step), step)
        downs = [
            late_ref[2 * unit * index + unit : 2 * unit * (index + 1), cols]
            for index in range(count)
        ]
        down = jnp.concatenate([down_ref[:, cols]] + downs, axis=0)
        out_ref[:, cols] = jnp.dot(hidden_ref[...], down, preferred_element_type=jnp.float32)
        return 0

    lax.fori_loop(0, width // step, body, 0)


def most_call(ids, own, other, combine, late, stacked):
    unit = late[0].shape[0] // 2
    half, width = own.shape
    hidden = stacked[2].shape[0] + len(late) * unit
    operands = [ids, own, other, *combine, *late, *stacked]
    return pl.pallas_call(
        lambda *refs: most_kernel(len(late), unit, *refs),
        out_shape=pltpu.VMEM((2 * half, width), jnp.float32),
        in_specs=specs(SMEM, 1)
        + specs(HBM, 2)
        + specs(VMEM, 2)
        + specs(HBM, len(late))
        + specs(VMEM, 5),
        out_specs=pl.BlockSpec(memory_space=VMEM),
        scratch_shapes=[
            pltpu.VMEM((2 * half, width), jnp.bfloat16),
            pltpu.VMEM((2 * unit * len(late), width), jnp.bfloat16),
            pltpu.VMEM((2 * half, hidden), jnp.bfloat16),
            pltpu.SemaphoreType.DMA((2 + len(late),)),
        ],
        cost_estimate=pl.CostEstimate(
            flops=2 * 2 * half * width * 3 * hidden,
            bytes_accessed=16 * MIB,
            transcendentals=2 * half * hidden,
        ),
        compiler_params=pltpu.CompilerParams(vmem_limit_bytes=14 * MIB),
        name="experts_most",
    )(*operands)


def rest_kernel(unit, ids_ref, one_ref, two_ref, near_ref, far_ref, gate_ref, up_ref, down_ref, most_ref, own_ref, send_ref, x_ref, both_ref, d_ref, sem):
    half = one_ref.shape[0]
    copies = grouped(
        [
            pltpu.make_async_copy(one_ref, x_ref.at[pl.ds(0, half)], sem.at[0]),
            pltpu.make_async_copy(two_ref, x_ref.at[pl.ds(half, half)], sem.at[1]),
            pltpu.make_async_copy(up_ref, both_ref.at[pl.ds(unit, unit)], sem.at[2]),
            pltpu.make_async_copy(down_ref, d_ref, sem.at[3]),
        ]
    )
    used = gate_ref.shape[0] - unit
    both_ref[:unit] = gate_ref[used:]
    for copy in copies[:3]:
        copy.wait()
    both = dot_nt(x_ref[...], both_ref[...])
    gate, up = both[:, :unit], both[:, unit:]
    combine = jnp.concatenate([near_ref[...], far_ref[...]], axis=0)
    scale = spread(ids_ref, combine, used // unit, 1, unit)
    hidden = (silu(gate) * up * scale).astype(jnp.bfloat16)
    copies[3].wait()
    width = most_ref.shape[1]
    step = math.gcd(width, 512)

    def body(at, _):
        cols = pl.ds(pl.multiple_of(at * step, step), step)
        out = most_ref[:, cols] + jnp.dot(
            hidden, d_ref[:, cols], preferred_element_type=jnp.float32
        )
        own_ref[:, cols] = out[:half]
        send_ref[:, cols] = out[half:].astype(jnp.bfloat16)
        return 0

    lax.fori_loop(0, width // step, body, 0)


def rest_call(ids, own, other, combine, gate, up, down, most):
    unit = up.shape[0]
    half, width = own.shape
    return pl.pallas_call(
        lambda *refs: rest_kernel(unit, *refs),
        out_shape=[
            pltpu.VMEM((half, width), jnp.float32),
            jax.ShapeDtypeStruct((half, width), jnp.bfloat16),
        ],
        in_specs=specs(SMEM, 1)
        + specs(HBM, 2)
        + specs(VMEM, 3)
        + specs(HBM, 2)
        + specs(VMEM, 1),
        out_specs=specs(VMEM, 2),
        scratch_shapes=[
            pltpu.VMEM((2 * half, width), jnp.bfloat16),
            pltpu.VMEM((2 * unit, width), jnp.bfloat16),
            pltpu.VMEM((unit, width), jnp.bfloat16),
            pltpu.SemaphoreType.DMA((4,)),
        ],
        cost_estimate=pl.CostEstimate(
            flops=2 * 2 * half * width * 3 * unit,
            bytes_accessed=10 * MIB,
            transcendentals=2 * half * unit,
        ),
        compiler_params=pltpu.CompilerParams(vmem_limit_bytes=10 * MIB),
        name="experts_rest",
    )(ids, own, other, *combine, gate, up, down, most)


def norm_rows(resid, gain):
    stream = resid.astype(jnp.float32)
    return (
        stream * lax.rsqrt(jnp.mean(stream * stream, axis=-1, keepdims=True) + 1e-06) * gain
    ).astype(jnp.bfloat16)


def ring_step(ahead, back, pairs):
    ahead = lax.ppermute(ahead, "sp", pairs[0])
    back = lax.ppermute(back, "sp", pairs[1])
    return ahead, back


def ring_gather(block, count):
    pairs = ring_pairs(count)
    out = [block]
    ahead = back = block
    for _ in range(1, count // 2):
        ahead, back = ring_step(ahead, back, pairs)
        out += [ahead, back]
    half = block.shape[0] // 2
    low, high = ring_step(ahead[:half], back[half:], pairs)
    return out, low, high


def swap(rows, pairs):
    return lax.ppermute(rows, "tp", pairs)


def fast_local(
    stream_in,
    q_first,
    q_second,
    k_first,
    k_second,
    values,
    head_lambda,
    w_out,
    norm_gain,
    routes,
    route_w,
    w_gate,
    w_up,
    w_down,
    s_gate,
    s_up,
    s_down,
):
    count = lax.axis_size("sp")
    members = lax.axis_size("tp")
    me = lax.axis_index("sp")
    mine = lax.axis_index("tp")
    seq_rows = q_first.shape[0]
    own_rows = seq_rows // members
    experts = w_gate.shape[0] * count
    unit = w_gate.shape[2] // members
    cores = [(t, t ^ 1) for t in range(members)]
    sides = [(t, t ^ 2) for t in range(members)]

    sources = jnp.asarray(ring_sources(count), jnp.int32)[me]
    ids = jnp.concatenate([jnp.stack([me, mine]).astype(jnp.int32), sources])
    kv = pack_call(k_first, k_second, values)
    blocks, low, high = ring_gather(kv, count)
    gate, rest = slices_call(ids, w_gate[0], w_up[0], w_down[0], unit)
    gates, gate_low, gate_high = ring_gather(gate, count)
    rests, rest_up, rest_down = ring_gather(rest, count)

    queries = (q_first, q_second)
    state = None
    for step in range(1, count // 2):
        begin, end = (0 if step == 1 else 2 * step - 1), 2 * step + 1
        spans = tuple((place, 1) for place in range(begin, end))
        result = attn_call(ids, *queries, blocks[begin:end], spans, state, own_rows)
        if step == 1:
            queries = result[:2]
        state = result[-3:]
    own, send = attn_call(
        ids,
        *queries,
        [low, high],
        ((count - 1, 2), (count - 1, 0)),
        state,
        own_rows,
        head_lambda,
        w_out,
        stream_in,
    )

    combine = jnp.sum(
        jnp.where(
            routes[:, :, None] == jnp.arange(experts, dtype=jnp.int32)[None, None, :],
            route_w[:, :, None],
            0.0,
        ),
        axis=1,
    )
    across = swap(combine, sides)
    paired = jnp.concatenate([combine, across])
    combine = (paired, swap(paired, cores))

    met = swap(send, cores)
    pair = (own + met.astype(jnp.float32)).astype(jnp.bfloat16)
    met = swap(pair, sides)
    stacked = stack_call([*gates, gate_low, gate_high], rests[:5], s_gate, s_up, s_down)
    resid = (
        pair.astype(jnp.float32)
        + jnp.concatenate([met[own_rows:], met[:own_rows]]).astype(jnp.float32)
    ).astype(jnp.bfloat16)
    resid = lax.optimization_barrier(resid)
    normed = norm_rows(resid, norm_gain)
    other = swap(normed, cores)
    most = most_call(ids, normed, other, combine, rests[5:], stacked)
    own, send = rest_call(
        ids, normed, other, combine, stacked[0], rest_up, rest_down, most
    )
    met = swap(send, cores)
    terms = own + met.astype(jnp.float32)
    met = swap(terms[own_rows:].astype(jnp.bfloat16), sides)
    return (
        resid[:own_rows].astype(jnp.float32) + terms[:own_rows] + met.astype(jnp.float32)
    ).astype(jnp.bfloat16)


def weights_travel(count, members, seq_rows, k_first, values, w_gate):
    unit = w_gate.shape[2] // members
    gathered = 3 * count * unit * w_gate.shape[1] * 2
    return (
        members == 4
        and count >= 4
        and count % 2 == 0
        and w_gate.shape[0] == 1
        and k_first.shape[1] == HEAD
        and values.shape[1] % 128 == 0
        and w_gate.shape[2] % (32 * members) == 0
        and seq_rows % (32 * members) == 0
        and count == 8
        and gathered <= 16 * 1024 * 1024
    )


def local(*args):
    count, members = lax.axis_size("sp"), lax.axis_size("tp")
    if weights_travel(count, members, args[1].shape[0], args[3], args[5], args[11]):
        return fast_local(*args)
    return slow_local(*args)


def solution(mesh):
    return jax.shard_map(
        local,
        mesh=mesh,
        in_specs=(
            P(("sp", "tp"), None),
            P("sp", "tp"),
            P("sp", "tp"),
            P("sp", "tp"),
            P("sp", "tp"),
            P("sp", "tp"),
            P("tp"),
            P("tp", None),
            P(),
            P(("sp", "tp"), None),
            P(("sp", "tp"), None),
            P("sp", None, None),
            P("sp", None, None),
            P("sp", None, None),
            P(None, "tp"),
            P(None, "tp"),
            P("tp", None),
        ),
        out_specs=P(("sp", "tp"), None),
        check_vma=False,
    )
```

```python
import math

import jax
import jax.numpy as jnp
from jax import lax
from jax.experimental import pallas as pl
from jax.experimental.pallas import tpu as pltpu
from jax.sharding import PartitionSpec as P

HEAD = 128
TURNS = (0, 2, 1, 3)


FLOOR = -1e30


def absorb(state, first_q, second_q, first_k, second_k, value_rows, query_pos, key_pos):
    allowed = key_pos[None, :] <= query_pos[:, None]
    scale = first_q.shape[-1] ** (-0.5)
    result = []
    pairs = ((first_q, first_k), (second_q, second_k))
    for index in range(2):
        query_rows, key_rows = pairs[index]
        peak, total, accum = (state[3 * index], state[3 * index + 1], state[3 * index + 2])
        scores = (
            jnp.einsum("qagd,kad->agqk", query_rows, key_rows, preferred_element_type=jnp.float32)
            * scale
        )
        scores = jnp.where(allowed, scores, FLOOR)
        raised = jnp.maximum(peak, scores.max(-1))
        weights = jnp.where(allowed, jnp.exp(scores - raised[..., None]), 0.0)
        fade = jnp.exp(peak - raised)
        total = total * fade + weights.sum(-1)
        accum = accum * fade[..., None] + jnp.einsum(
            "agqk,kad->agqd",
            weights.astype(jnp.bfloat16),
            value_rows,
            preferred_element_type=jnp.float32,
        )
        result += [raised, total, accum]
    return tuple(result)


def empty_state(kv_local, group, count, value_dim):
    peaks = jnp.full((kv_local, group, count), FLOOR, jnp.float32)
    sums = jnp.zeros((kv_local, group, count), jnp.float32)
    accums = jnp.zeros((kv_local, group, count, value_dim), jnp.float32)
    return (peaks, sums, accums, peaks, sums, accums)


def fold_rows(state, first_q, second_q, query_pos, last_row, pieces, start):
    first_k, second_k, value_rows = pieces
    length = first_k.shape[0]
    kv_local = first_q.shape[1]
    value_dim = value_rows.shape[1] // kv_local
    span = math.gcd(length, 2048)

    def sweep(current):

        def visit(block, inner):
            begin = block * span
            key_one = lax.dynamic_slice_in_dim(first_k, begin, span, 0).reshape(
                span, kv_local, HEAD
            )
            key_two = lax.dynamic_slice_in_dim(second_k, begin, span, 0).reshape(
                span, kv_local, HEAD
            )
            value_part = lax.dynamic_slice_in_dim(value_rows, begin, span, 0).reshape(
                span, kv_local, value_dim
            )
            key_pos = begin + jnp.arange(span, dtype=jnp.int32)
            return absorb(
                inner, first_q, second_q, key_one, key_two, value_part, query_pos, key_pos
            )

        return lax.fori_loop(0, length // span, visit, current)

    def unchanged(current):
        return current

    return lax.cond(start <= last_row, sweep, unchanged, state)


def finish_heads(final, head_lambda):
    kv_local, group, count, value_dim = final[2].shape
    weight = head_lambda.reshape(kv_local, group, 1, 1)
    head_out = final[2] / final[1][..., None] - weight * final[5] / final[4][..., None]
    head_out = head_out * lax.rsqrt(jnp.mean(head_out * head_out, axis=-1, keepdims=True) + 1e-05)
    return (
        head_out.transpose(2, 0, 1, 3)
        .reshape(count, kv_local * group * value_dim)
        .astype(jnp.bfloat16)
    )


def shared_part(normed, s_gate, s_up, s_down):
    piece = lax.all_gather(normed, "tp", axis=0, tiled=True)
    gate_part = jnp.dot(piece, s_gate, preferred_element_type=jnp.float32)
    up_part = jnp.dot(piece, s_up, preferred_element_type=jnp.float32)
    hidden = (jax.nn.silu(gate_part) * up_part).astype(jnp.bfloat16)
    terms = jnp.dot(hidden, s_down, preferred_element_type=jnp.float32)
    return lax.psum_scatter(
        terms.astype(jnp.bfloat16), "tp", scatter_dimension=0, tiled=True
    ).astype(jnp.float32)


def routed_part(normed, routes, route_w, w_gate, w_up, w_down):
    rows, topk = routes.shape
    local_experts = w_gate.shape[0]
    experts = local_experts * lax.axis_size("sp")
    slots = max(2, 3 * rows * topk // (2 * experts))
    flat_ids = routes.reshape(-1)
    hits = (flat_ids[:, None] == jnp.arange(experts, dtype=jnp.int32)[None, :]).astype(jnp.int32)
    slot_of = jnp.sum(jnp.cumsum(hits, axis=0) * hits, axis=1) - 1
    target = flat_ids * slots + slot_of
    placing = jnp.any(
        jnp.arange(experts * slots, dtype=jnp.int32)[:, None, None]
        == target.reshape(rows, topk)[None, :, :],
        axis=-1,
    ).astype(jnp.bfloat16)
    outgoing = (
        jnp.dot(placing, normed, preferred_element_type=jnp.float32)
        .astype(jnp.bfloat16)
        .reshape(experts, slots, normed.shape[1])
    )
    arrived = lax.all_to_all(outgoing, "sp", split_axis=0, concat_axis=0, tiled=True)
    sources = arrived.shape[0] // local_experts
    grouped = arrived.reshape(sources, local_experts, arrived.shape[1], arrived.shape[2])
    gate_part = jnp.einsum("sjcd,jdf->sjcf", grouped, w_gate, preferred_element_type=jnp.float32)
    up_part = jnp.einsum("sjcd,jdf->sjcf", grouped, w_up, preferred_element_type=jnp.float32)
    hidden = (jax.nn.silu(gate_part) * up_part).astype(jnp.bfloat16)
    result = jnp.einsum(
        "sjcf,jfd->sjcd", hidden, w_down, preferred_element_type=jnp.float32
    ).astype(jnp.bfloat16)
    returned = lax.all_to_all(
        result.reshape(arrived.shape), "sp", split_axis=0, concat_axis=0, tiled=True
    )
    picked = (
        returned.reshape(experts * slots, normed.shape[1])[target]
        .reshape(rows, topk, normed.shape[1])
        .astype(jnp.float32)
    )
    return jnp.sum(picked * route_w[..., None], axis=1)


def slow_local(
    stream_in,
    q_first,
    q_second,
    k_first,
    k_second,
    values,
    head_lambda,
    w_out,
    norm_gain,
    routes,
    route_w,
    w_gate,
    w_up,
    w_down,
    s_gate,
    s_up,
    s_down,
):
    seq_rows = q_first.shape[0]
    kv_local = k_first.shape[1] // HEAD
    heads_local = q_first.shape[1] // HEAD
    group = heads_local // kv_local
    value_dim = values.shape[1] // kv_local
    offset = lax.axis_index("sp") * seq_rows
    query_pos = offset + jnp.arange(seq_rows, dtype=jnp.int32)
    last_row = offset + seq_rows - 1
    first_q = q_first.reshape(seq_rows, kv_local, group, HEAD)
    second_q = q_second.reshape(seq_rows, kv_local, group, HEAD)
    start_state = empty_state(kv_local, group, seq_rows, value_dim)
    folded_state = fold_rows(
        start_state,
        first_q,
        second_q,
        query_pos,
        last_row,
        (
            lax.all_gather(k_first, "sp", axis=0, tiled=True),
            lax.all_gather(k_second, "sp", axis=0, tiled=True),
            lax.all_gather(values, "sp", axis=0, tiled=True),
        ),
        jnp.int32(0),
    )
    attn_rows = finish_heads(folded_state, head_lambda)
    attn = lax.psum_scatter(
        jnp.dot(attn_rows, w_out, preferred_element_type=jnp.float32).astype(jnp.bfloat16),
        "tp",
        scatter_dimension=0,
        tiled=True,
    ).astype(jnp.float32)
    resid = (stream_in.astype(jnp.float32) + attn).astype(jnp.bfloat16)
    stream = lax.optimization_barrier(resid).astype(jnp.float32)
    normed = (
        stream * lax.rsqrt(jnp.mean(stream * stream, axis=-1, keepdims=True) + 1e-06) * norm_gain
    ).astype(jnp.bfloat16)
    routed = routed_part(normed, routes, route_w, w_gate, w_up, w_down)
    shared = shared_part(normed, s_gate, s_up, s_down)
    return (stream + routed + shared).astype(jnp.bfloat16)


VMEM = pltpu.MemorySpace.VMEM
MIB = 1024 * 1024
SMEM = pltpu.MemorySpace.SMEM
HBM = pltpu.MemorySpace.HBM


def ring_order(count):
    return list(range(0, count, 2)) + list(range(count - 1, 0, -2))


def ring_pairs(count):
    order = ring_order(count)
    forward = [(order[i], order[(i + 1) % count]) for i in range(count)]
    return forward, [(b, a) for a, b in forward]


def ring_sources(count):
    order = ring_order(count)
    rows = [None] * count
    for place, index in enumerate(order):
        row = [index]
        for step in range(1, count // 2):
            row += [order[(place - step) % count], order[(place + step) % count]]
        row.append(order[(place + count // 2) % count])
        rows[index] = row
    return rows


def dot_nt(a, b):
    return lax.dot_general(a, b, (((1,), (1,)), ((), ())), preferred_element_type=jnp.float32)


def grouped(copies):
    for copy in copies:
        copy.start()
    return copies


def attn_kernel(spans, first, last, scale, own_rows, *refs):
    refs = list(refs)
    ids_ref = refs.pop(0)
    if last:
        lam_ref = refs.pop(0)
    q_in = [refs.pop(0), refs.pop(0)]
    kv_in = [refs.pop(0) for _ in spans]
    if not first:
        state_in = [refs.pop(0) for _ in range(3)]
    if last:
        w_ref, stream_ref = refs.pop(0), refs.pop(0)
        own_ref, send_ref, m_ref, l_ref, acc_ref, mixed_ref, w, stream, w_sem = refs[:9]
        del refs[:9]
        load = pltpu.make_async_copy(w_ref, w, w_sem.at[0])
        feed = pltpu.make_async_copy(stream_ref, stream, w_sem.at[1])
    elif first:
        q_refs = [refs.pop(0), refs.pop(0)]
        m_ref, l_ref, acc_ref = refs.pop(0), refs.pop(0), refs.pop(0)
    else:
        m_ref, l_ref, acc_ref = refs.pop(0), refs.pop(0), refs.pop(0)
    kv_scratch, sem = refs
    rows = q_in[0].shape[0]
    heads = q_in[0].shape[1] // HEAD
    parts = rows // own_rows
    me, mine = ids_ref[0], ids_ref[1]
    outs = (m_ref, l_ref, acc_ref)
    starts = [sum(b.shape[0] for b in kv_in[:at]) for at in range(len(spans))]
    kv_refs = [
        kv_scratch.at[pl.ds(start, ref.shape[0])] for start, ref in zip(starts, kv_in)
    ]
    copies = grouped(
        [
            pltpu.make_async_copy(source, into, sem.at[at])
            for at, (source, into) in enumerate(zip(kv_in, kv_refs))
        ]
    )
    if last:
        load.start()
        feed.start()
    if first:
        loads = grouped(
            [
                pltpu.make_async_copy(
                    q_in[which].at[
                        pl.ds(pl.multiple_of((mine ^ turn) * own_rows, own_rows), own_rows)
                    ],
                    q_refs[which].at[pl.ds(index * own_rows, own_rows)],
                    sem.at[len(spans) + which * parts + index],
                )
                for which in range(2)
                for index, turn in enumerate(TURNS)
            ]
        )
        for copy in loads:
            copy.wait()
    else:
        q_refs = q_in

    def fold(kv_ref, diagonal, old_refs=outs):
        keys = kv_ref.shape[0]
        v = kv_ref[:, 2 * HEAD :]
        old_m, old_l, old_acc = old_refs
        if diagonal:
            row_at = lax.broadcasted_iota(jnp.int32, (rows, keys), 0)
            key_at = lax.broadcasted_iota(jnp.int32, (rows, keys), 1)
            part = row_at // own_rows
            place = jnp.zeros_like(part)
            for index, turn in enumerate(TURNS):
                place = jnp.where(part == index, mine ^ turn, place)
            allowed = key_at <= place * own_rows + row_at % own_rows
        for head in range(heads):
            for which in range(2):
                pair = 2 * head + which
                q = q_refs[which][:, head * HEAD : (head + 1) * HEAD]
                k = kv_ref[:, which * HEAD : (which + 1) * HEAD]
                s = dot_nt(q, k)
                if diagonal:
                    s = jnp.where(allowed, s, FLOOR)
                top = jnp.max(s, axis=1, keepdims=True)
                if diagonal:
                    raised = jnp.broadcast_to(top, (rows, 128))
                else:
                    old = old_m[pair]
                    raised = jnp.maximum(old, top)
                wide = jnp.concatenate([raised] * (keys // 128), axis=1)
                p = jnp.exp((s - wide) * scale)
                part_sum = p[:, :128]
                for at in range(128, keys, 128):
                    part_sum = part_sum + p[:, at : at + 128]
                prod = jnp.dot(p.astype(jnp.bfloat16), v, preferred_element_type=jnp.float32)
                m_ref[pair] = raised
                if diagonal:
                    l_ref[pair] = part_sum
                    acc_ref[pair] = prod
                else:
                    fade = jnp.exp((old - raised) * scale)
                    l_ref[pair] = old_l[pair] * fade + part_sum
                    fades = jnp.concatenate([fade] * (prod.shape[1] // 128), axis=1)
                    acc_ref[pair] = old_acc[pair] * fades + prod

    for index, (place, pieces) in enumerate(spans):
        copies[index].wait()
        if pieces == 2:
            copies[index + 1].wait()
            kv_ref = kv_scratch.at[
                pl.ds(starts[index], kv_in[index].shape[0] + kv_in[index + 1].shape[0])
            ]
        elif pieces == 0:
            continue
        else:
            kv_ref = kv_refs[index]
        if first and index == 0:
            fold(kv_ref, True)
            continue
        earlier = ids_ref[2 + place] < me
        carry = not first and index == 0

        @pl.when(earlier)
        def _(kv_ref=kv_ref, carry=carry):
            fold(kv_ref, False, state_in if carry else outs)

        if carry:

            @pl.when(jnp.logical_not(earlier))
            def _():
                for into, source in zip(outs, state_in):
                    into[...] = source[...]

        if pieces == 2:
            break

    if last:
        for head in range(heads):
            terms = []
            for which in range(2):
                pair = 2 * head + which
                total = jnp.sum(l_ref[pair], axis=1, keepdims=True)
                terms.append(acc_ref[pair] / total)
            mixed = terms[0] - lam_ref[head] * terms[1]
            square = jnp.mean(mixed * mixed, axis=1, keepdims=True)
            mixed = mixed * lax.rsqrt(square + 1e-05)
            width = mixed.shape[1]
            mixed_ref[:, head * width : (head + 1) * width] = mixed.astype(jnp.bfloat16)
        load.wait()
        feed.wait()
        half = rows // 2
        step = math.gcd(w.shape[1], 512)

        def body(at, _):
            cols = pl.ds(pl.multiple_of(at * step, step), step)
            out = jnp.dot(mixed_ref[...], w[:, cols], preferred_element_type=jnp.float32)
            own_ref[:own_rows, cols] = out[:own_rows] + stream[:, cols].astype(jnp.float32)
            own_ref[own_rows:, cols] = out[own_rows:half]
            send_ref[:, cols] = out[half:].astype(jnp.bfloat16)
            return 0

        lax.fori_loop(0, w.shape[1] // step, body, 0)


def specs(space, count):
    return [pl.BlockSpec(memory_space=space)] * count


def attn_call(ids, q_first, q_second, blocks, spans, state, own_rows, lam=None, w_out=None, stream_in=None):
    rows = q_first.shape[0]
    heads = q_first.shape[1] // HEAD
    value_dim = blocks[0].shape[1] - 2 * HEAD
    first, last = state is None, w_out is not None
    states = [
        pltpu.VMEM((2 * heads, rows, 128), jnp.float32),
        pltpu.VMEM((2 * heads, rows, 128), jnp.float32),
        pltpu.VMEM((2 * heads, rows, value_dim), jnp.float32),
    ]
    operands = [ids] + ([lam] if last else []) + [q_first, q_second, *blocks]
    in_specs = specs(SMEM, 2 if last else 1)
    in_specs += specs(HBM if first else VMEM, 2) + specs(HBM, len(blocks))
    if not first:
        operands += list(state)
        in_specs += specs(VMEM, 3)
    scratch = []
    if last:
        operands += [w_out, stream_in]
        in_specs += specs(HBM, 2)
        width = w_out.shape[1]
        out_shape = [
            pltpu.VMEM((rows // 2, width), jnp.float32),
            jax.ShapeDtypeStruct((rows // 2, width), jnp.bfloat16),
        ]
        scratch = [
            *states,
            pltpu.VMEM((rows, heads * value_dim), jnp.bfloat16),
            pltpu.VMEM(w_out.shape, jnp.bfloat16),
            pltpu.VMEM(stream_in.shape, jnp.bfloat16),
            pltpu.SemaphoreType.DMA((2,)),
        ]
    else:
        out_shape = list(states)
        if first:
            out_shape = [pltpu.VMEM(q_first.shape, q_first.dtype)] * 2 + out_shape
    keys = sum(b.shape[0] for b in blocks)
    scratch += [
        pltpu.VMEM((keys, blocks[0].shape[1]), jnp.bfloat16),
        pltpu.SemaphoreType.DMA((len(blocks) + 2 * rows // own_rows,)),
    ]
    body = lambda *refs: attn_kernel(spans, first, last, HEAD**-0.5, own_rows, *refs)
    return pl.pallas_call(
        body,
        out_shape=out_shape,
        in_specs=in_specs,
        out_specs=specs(VMEM, len(out_shape)),
        scratch_shapes=scratch,
        cost_estimate=pl.CostEstimate(
            flops=8 * heads * rows * keys * (HEAD + value_dim),
            bytes_accessed=4 * 1024 * 1024,
            transcendentals=2 * heads * rows * keys,
        ),
        compiler_params=pltpu.CompilerParams(vmem_limit_bytes=(22 if last else 12) * MIB),
    )(*operands)


def pack_kernel(one_ref, two_ref, three_ref, out_ref, sem):
    wide = one_ref.shape[1]
    cuts = ((0, wide), (wide, wide), (2 * wide, three_ref.shape[1]))
    copies = grouped(
        [
            pltpu.make_async_copy(ref, out_ref.at[:, pl.ds(start, size)], sem.at[at])
            for at, (ref, (start, size)) in enumerate(zip((one_ref, two_ref, three_ref), cuts))
        ]
    )
    for copy in copies:
        copy.wait()


def pack_call(one, two, three):
    width = one.shape[1] + two.shape[1] + three.shape[1]
    return pl.pallas_call(
        pack_kernel,
        out_shape=jax.ShapeDtypeStruct((one.shape[0], width), one.dtype),
        in_specs=specs(HBM, 3),
        out_specs=pl.BlockSpec(memory_space=VMEM),
        scratch_shapes=[pltpu.SemaphoreType.DMA((3,))],
        name="pack",
    )(one, two, three)


def slices_kernel(unit, at_ref, gate_ref, up_ref, down_ref, gate_out, up_out, down_out, gate, up, turned, sem):
    start = pl.multiple_of(at_ref[0] * unit, unit)
    loads = grouped(
        [
            pltpu.make_async_copy(gate_ref, gate, sem.at[0]),
            pltpu.make_async_copy(up_ref, up, sem.at[1]),
            pltpu.make_async_copy(down_ref.at[pl.ds(start, unit)], down_out, sem.at[2]),
        ]
    )
    for load, source, out in ((loads[0], gate, gate_out), (loads[1], up, up_out)):
        load.wait()
        turned[...] = source[...].T
        out[...] = turned[pl.ds(start, unit)]
    loads[2].wait()


def slices_call(mine, gate, up, down, unit):
    width = gate.shape[0]
    return pl.pallas_call(
        lambda *refs: slices_kernel(unit, *refs),
        out_shape=[jax.ShapeDtypeStruct((unit, width), gate.dtype)] * 3,
        in_specs=specs(SMEM, 1) + specs(HBM, 3),
        out_specs=specs(VMEM, 3),
        scratch_shapes=[
            pltpu.VMEM(gate.shape, gate.dtype),
            pltpu.VMEM(up.shape, gate.dtype),
            pltpu.VMEM((gate.shape[1], width), gate.dtype),
            pltpu.SemaphoreType.DMA((3,)),
        ],
        name="slices",
    )(mine, gate, up, down)


def combine_kernel(routes_ref, weights_ref, out_ref):
    expert = lax.broadcasted_iota(jnp.int32, out_ref.shape, 1)
    total = jnp.zeros(out_ref.shape, jnp.float32)
    for choice in range(routes_ref.shape[1]):
        chosen = jnp.broadcast_to(routes_ref[:, choice : choice + 1], out_ref.shape)
        weight = jnp.broadcast_to(weights_ref[:, choice : choice + 1], out_ref.shape)
        total += jnp.where(expert == chosen, weight, 0.0)
    out_ref[...] = total


def combine_call(routes, weights):
    return pl.pallas_call(
        combine_kernel,
        out_shape=jax.ShapeDtypeStruct((routes.shape[0], 128), jnp.float32),
        in_specs=specs(VMEM, 2),
        out_specs=pl.BlockSpec(memory_space=VMEM),
        compiler_params=pltpu.CompilerParams(vmem_limit_bytes=2 * MIB),
        name="combine",
    )(routes, weights)


def silu(v):
    return v / (1.0 + jnp.exp(-v))


def spread(ids_ref, combine, count, unit):
    expert = lax.broadcasted_iota(jnp.int32, combine.shape, 1)
    columns = []
    for block in range(count):
        picked = jnp.where(expert == ids_ref[2 + block], combine, 0.0)
        column = jnp.sum(picked, axis=1, keepdims=True)
        columns.append(jnp.broadcast_to(column, (combine.shape[0], unit)))
    return jnp.concatenate(columns, axis=1)


def stack_kernel(plan, *refs):
    sem = refs[-1]
    outs = refs[-1 - len(plan) : -1]
    copies = []
    for out, pieces in zip(outs, plan):
        at = 0
        for which, first, rows in pieces:
            copies.append(
                pltpu.make_async_copy(
                    refs[which].at[pl.ds(first, rows)],
                    out.at[pl.ds(at, rows)],
                    sem.at[len(copies)],
                )
            )
            at += rows
    for copy in grouped(copies):
        copy.wait()


def whole(array):
    return (array, 0, array.shape[0])


def stack_call(*groups):
    operands, plan, shapes = [], [], []
    for group in groups:
        pieces = []
        for array, first, rows in group:
            pieces.append((len(operands), first, rows))
            operands.append(array)
        plan.append(tuple(pieces))
        shapes.append((sum(rows for _, _, rows in group), group[0][0].shape[1]))
    return pl.pallas_call(
        lambda *refs: stack_kernel(tuple(plan), *refs),
        out_shape=[pltpu.VMEM(shape, operands[0].dtype) for shape in shapes],
        in_specs=specs(HBM, len(operands)),
        out_specs=specs(VMEM, len(groups)),
        scratch_shapes=[pltpu.SemaphoreType.DMA((len(operands),))],
        cost_estimate=pl.CostEstimate(flops=10**9, bytes_accessed=16 * MIB, transcendentals=0),
        compiler_params=pltpu.CompilerParams(vmem_limit_bytes=2 * MIB),
        name="stack",
    )(*operands)


def hidden_kernel(unit, ids_ref, one_ref, two_ref, near_ref, far_ref, low_ref, high_ref, gate_ref, up_ref, sg_ref, su_ref, out_ref, x_ref, late_ref, sem):
    half = one_ref.shape[0]
    cut = low_ref.shape[0]
    copies = grouped(
        [
            pltpu.make_async_copy(one_ref, x_ref.at[pl.ds(0, half)], sem.at[0]),
            pltpu.make_async_copy(two_ref, x_ref.at[pl.ds(half, half)], sem.at[1]),
            pltpu.make_async_copy(low_ref, late_ref.at[pl.ds(0, cut)], sem.at[2]),
            pltpu.make_async_copy(high_ref, late_ref.at[pl.ds(cut, high_ref.shape[0])], sem.at[3]),
        ]
    )
    for copy in copies:
        copy.wait()
    x = x_ref[...]
    gate = dot_nt(x, gate_ref[...])
    up = dot_nt(x, jnp.concatenate([up_ref[...], late_ref[...]], axis=0))
    count = gate.shape[1] // unit
    combine = jnp.concatenate([near_ref[...], far_ref[...]], axis=0)
    hidden = silu(gate) * up * spread(ids_ref, combine, count, unit)
    gate = jnp.dot(x, sg_ref[...], preferred_element_type=jnp.float32)
    up = jnp.dot(x, su_ref[...], preferred_element_type=jnp.float32)
    wide = gate.shape[1]
    out_ref[:, :wide] = (silu(gate) * up).astype(jnp.bfloat16)
    out_ref[:, wide:] = hidden.astype(jnp.bfloat16)


def hidden_call(ids, own, other, combine, low, high, gate, up, s_gate, s_up, unit):
    half, width = own.shape
    total = s_gate.shape[1] + up.shape[0] + unit
    return pl.pallas_call(
        lambda *refs: hidden_kernel(unit, *refs),
        out_shape=pltpu.VMEM((2 * half, total), jnp.bfloat16),
        in_specs=specs(SMEM, 1) + specs(HBM, 2) + specs(VMEM, 2) + specs(HBM, 2) + specs(VMEM, 4),
        out_specs=pl.BlockSpec(memory_space=VMEM),
        scratch_shapes=[
            pltpu.VMEM((2 * half, width), jnp.bfloat16),
            pltpu.VMEM((unit, width), jnp.bfloat16),
            pltpu.SemaphoreType.DMA((4,)),
        ],
        cost_estimate=pl.CostEstimate(
            flops=2 * 2 * half * width * 2 * total,
            bytes_accessed=12 * MIB,
            transcendentals=2 * half * total,
        ),
        compiler_params=pltpu.CompilerParams(vmem_limit_bytes=10 * MIB),
        name="hidden",
    )(ids, own, other, *combine, low, high, gate, up, s_gate, s_up)


def down_kernel(first, hidden_ref, most_ref, low_ref, high_ref, own_ref, send_ref, late_ref, sem):
    half, width = own_ref.shape
    rows = low_ref.shape[0]
    copies = grouped(
        [
            pltpu.make_async_copy(
                ref.at[:, pl.ds(first, width)], late_ref.at[pl.ds(at * rows, rows)], sem.at[at]
            )
            for at, ref in enumerate((low_ref, high_ref))
        ]
    )
    for copy in copies:
        copy.wait()
    step = math.gcd(width, 512)
    for at in range(0, width, step):
        down = jnp.concatenate(
            [most_ref[:, first + at : first + at + step], late_ref[:, at : at + step]], axis=0
        )
        out = jnp.dot(hidden_ref[...], down, preferred_element_type=jnp.float32)
        own_ref[:, at : at + step] = out[:half]
        send_ref[:, at : at + step] = out[half:].astype(jnp.bfloat16)


def down_call(hidden, most, low, high, first, width):
    rows = hidden.shape[0]
    return pl.pallas_call(
        lambda *refs: down_kernel(first, *refs),
        out_shape=[
            pltpu.VMEM((rows // 2, width), jnp.float32),
            jax.ShapeDtypeStruct((rows // 2, width), jnp.bfloat16),
        ],
        in_specs=specs(VMEM, 2) + specs(HBM, 2),
        out_specs=specs(VMEM, 2),
        scratch_shapes=[
            pltpu.VMEM((2 * low.shape[0], width), jnp.bfloat16),
            pltpu.SemaphoreType.DMA((2,)),
        ],
        cost_estimate=pl.CostEstimate(
            flops=2 * rows * width * hidden.shape[1], bytes_accessed=8 * MIB, transcendentals=0
        ),
        compiler_params=pltpu.CompilerParams(vmem_limit_bytes=6 * MIB),
    )(hidden, most, low, high)


def final_kernel(resid_ref, *refs):
    out_ref, met, sem = refs[-3:]
    parts = refs[: -3]
    count = len(parts) // 2
    rows = out_ref.shape[0]
    width = met.shape[2]
    copies = grouped(
        [
            pltpu.make_async_copy(parts[2 * at + 1], met.at[at], sem.at[at])
            for at in range(count)
        ]
    )
    for at in range(count):
        copies[at].wait()
        cols = slice(at * width, (at + 1) * width)
        total = resid_ref[:rows, cols].astype(jnp.float32) + parts[2 * at][:rows]
        out_ref[:, cols] = (total + met[at].astype(jnp.float32)).astype(jnp.bfloat16)


def final_call(resid, parts, rows):
    width = parts[0][1].shape[1]
    operands = [resid] + [array for part in parts for array in part]
    return pl.pallas_call(
        final_kernel,
        out_shape=jax.ShapeDtypeStruct((rows, resid.shape[1]), jnp.bfloat16),
        in_specs=specs(VMEM, 1) + (specs(VMEM, 1) + specs(HBM, 1)) * len(parts),
        out_specs=pl.BlockSpec(memory_space=VMEM),
        scratch_shapes=[
            pltpu.VMEM((len(parts), rows, width), jnp.bfloat16),
            pltpu.SemaphoreType.DMA((len(parts),)),
        ],
        compiler_params=pltpu.CompilerParams(vmem_limit_bytes=6 * MIB),
        name="final",
    )(*operands)


def norm_rows(resid, gain):
    stream = resid.astype(jnp.float32)
    return (
        stream * lax.rsqrt(jnp.mean(stream * stream, axis=-1, keepdims=True) + 1e-06) * gain
    ).astype(jnp.bfloat16)


def ring_step(ahead, back, pairs):
    ahead = lax.ppermute(ahead, "sp", pairs[0])
    back = lax.ppermute(back, "sp", pairs[1])
    return ahead, back


def ring_gather(block, count):
    pairs = ring_pairs(count)
    out = [block]
    ahead = back = block
    for _ in range(1, count // 2):
        ahead, back = ring_step(ahead, back, pairs)
        out += [ahead, back]
    half = block.shape[0] // 2
    low, high = ring_step(ahead[:half], back[half:], pairs)
    return out, low, high


def swap(rows, pairs):
    return lax.ppermute(rows, "tp", pairs)


def fast_local(
    stream_in,
    q_first,
    q_second,
    k_first,
    k_second,
    values,
    head_lambda,
    w_out,
    norm_gain,
    routes,
    route_w,
    w_gate,
    w_up,
    w_down,
    s_gate,
    s_up,
    s_down,
):
    count = lax.axis_size("sp")
    members = lax.axis_size("tp")
    me = lax.axis_index("sp")
    mine = lax.axis_index("tp")
    seq_rows = q_first.shape[0]
    own_rows = seq_rows // members
    unit = w_gate.shape[2] // members
    cores = [(t, t ^ 1) for t in range(members)]
    sides = [(t, t ^ 2) for t in range(members)]

    sources = jnp.asarray(ring_sources(count), jnp.int32)[me]
    ids = jnp.concatenate([jnp.stack([me, mine]).astype(jnp.int32), sources])
    kv = pack_call(k_first, k_second, values)
    blocks, low, high = ring_gather(kv, count)
    gate, up, down = slices_call(mine[None].astype(jnp.int32), w_gate[0], w_up[0], w_down[0], unit)
    gates, gate_low, gate_high = ring_gather(gate, count)
    ups, up_low, up_high = ring_gather(up, count)
    downs, down_low, down_high = ring_gather(down, count)

    queries = (q_first, q_second)
    state = None
    for step in range(1, count // 2):
        begin, end = (0 if step == 1 else 2 * step - 1), 2 * step + 1
        spans = tuple((place, 1) for place in range(begin, end))
        result = attn_call(ids, *queries, blocks[begin:end], spans, state, own_rows)
        if step == 1:
            queries = result[:2]
        state = result[-3:]
    own, send = attn_call(
        ids,
        *queries,
        [low, high],
        ((count - 1, 2), (count - 1, 0)),
        state,
        own_rows,
        head_lambda,
        w_out,
        stream_in,
    )

    combine = combine_call(routes, route_w)
    across = swap(combine, sides)
    paired = jnp.concatenate([combine, across])
    combine = (paired, swap(paired, cores))

    met = swap(send, cores)
    pair = (own + met.astype(jnp.float32)).astype(jnp.bfloat16)
    met = swap(pair, sides)
    gate_all, sg, su = stack_call(
        [whole(block) for block in (*gates, gate_low, gate_high)],
        [whole(s_gate)],
        [whole(s_up)],
    )
    (up_most,) = stack_call([whole(block) for block in ups])
    resid = (
        pair.astype(jnp.float32)
        + jnp.concatenate([met[own_rows:], met[:own_rows]]).astype(jnp.float32)
    ).astype(jnp.bfloat16)
    resid = lax.optimization_barrier(resid)
    normed = norm_rows(resid, norm_gain)
    other = swap(normed, cores)
    hidden = hidden_call(
        ids, normed, other, combine, up_low, up_high, gate_all, up_most, sg, su, unit
    )
    (down_most,) = stack_call([whole(s_down)] + [whole(block) for block in downs])
    width = stream_in.shape[1] // 2
    sums = []
    for part in range(2):
        sums.append(down_call(hidden, down_most, down_low, down_high, part * width, width))
    parts = []
    for own, send in sums:
        met = swap(send, cores)
        terms = own + met.astype(jnp.float32)
        met = swap(terms[own_rows:].astype(jnp.bfloat16), sides)
        parts.append((terms, met))
    return final_call(resid, parts, own_rows)


def weights_travel(count, members, seq_rows, k_first, values, w_gate):
    unit = w_gate.shape[2] // members
    gathered = 3 * count * unit * w_gate.shape[1] * 2
    return (
        members == 4
        and count >= 4
        and count % 2 == 0
        and w_gate.shape[0] == 1
        and k_first.shape[1] == HEAD
        and values.shape[1] % 128 == 0
        and w_gate.shape[2] % (32 * members) == 0
        and seq_rows % (32 * members) == 0
        and count == 8
        and w_gate.shape[0] * count <= 128
        and gathered <= 16 * 1024 * 1024
    )


def local(*args):
    count, members = lax.axis_size("sp"), lax.axis_size("tp")
    if weights_travel(count, members, args[1].shape[0], args[3], args[5], args[11]):
        return fast_local(*args)
    return slow_local(*args)


def solution(mesh):
    return jax.shard_map(
        local,
        mesh=mesh,
        in_specs=(
            P(("sp", "tp"), None),
            P("sp", "tp"),
            P("sp", "tp"),
            P("sp", "tp"),
            P("sp", "tp"),
            P("sp", "tp"),
            P("tp"),
            P("tp", None),
            P(),
            P(("sp", "tp"), None),
            P(("sp", "tp"), None),
            P("sp", None, None),
            P("sp", None, None),
            P("sp", None, None),
            P(None, "tp"),
            P(None, "tp"),
            P("tp", None),
        ),
        out_specs=P(("sp", "tp"), None),
        check_vma=False,
    )
```

```python
import math

import jax
import jax.numpy as jnp
from jax import lax
from jax.experimental import pallas as pl
from jax.experimental.pallas import tpu as pltpu
from jax.sharding import PartitionSpec as P

HEAD = 128
TURNS = (0, 2, 1, 3)


FLOOR = -1e30


def absorb(state, first_q, second_q, first_k, second_k, value_rows, query_pos, key_pos):
    allowed = key_pos[None, :] <= query_pos[:, None]
    scale = first_q.shape[-1] ** (-0.5)
    result = []
    pairs = ((first_q, first_k), (second_q, second_k))
    for index in range(2):
        query_rows, key_rows = pairs[index]
        peak, total, accum = (state[3 * index], state[3 * index + 1], state[3 * index + 2])
        scores = (
            jnp.einsum("qagd,kad->agqk", query_rows, key_rows, preferred_element_type=jnp.float32)
            * scale
        )
        scores = jnp.where(allowed, scores, FLOOR)
        raised = jnp.maximum(peak, scores.max(-1))
        weights = jnp.where(allowed, jnp.exp(scores - raised[..., None]), 0.0)
        fade = jnp.exp(peak - raised)
        total = total * fade + weights.sum(-1)
        accum = accum * fade[..., None] + jnp.einsum(
            "agqk,kad->agqd",
            weights.astype(jnp.bfloat16),
            value_rows,
            preferred_element_type=jnp.float32,
        )
        result += [raised, total, accum]
    return tuple(result)


def empty_state(kv_local, group, count, value_dim):
    peaks = jnp.full((kv_local, group, count), FLOOR, jnp.float32)
    sums = jnp.zeros((kv_local, group, count), jnp.float32)
    accums = jnp.zeros((kv_local, group, count, value_dim), jnp.float32)
    return (peaks, sums, accums, peaks, sums, accums)


def fold_rows(state, first_q, second_q, query_pos, last_row, pieces, start):
    first_k, second_k, value_rows = pieces
    length = first_k.shape[0]
    kv_local = first_q.shape[1]
    value_dim = value_rows.shape[1] // kv_local
    span = math.gcd(length, 2048)

    def sweep(current):

        def visit(block, inner):
            begin = block * span
            key_one = lax.dynamic_slice_in_dim(first_k, begin, span, 0).reshape(
                span, kv_local, HEAD
            )
            key_two = lax.dynamic_slice_in_dim(second_k, begin, span, 0).reshape(
                span, kv_local, HEAD
            )
            value_part = lax.dynamic_slice_in_dim(value_rows, begin, span, 0).reshape(
                span, kv_local, value_dim
            )
            key_pos = begin + jnp.arange(span, dtype=jnp.int32)
            return absorb(
                inner, first_q, second_q, key_one, key_two, value_part, query_pos, key_pos
            )

        return lax.fori_loop(0, length // span, visit, current)

    def unchanged(current):
        return current

    return lax.cond(start <= last_row, sweep, unchanged, state)


def finish_heads(final, head_lambda):
    kv_local, group, count, value_dim = final[2].shape
    weight = head_lambda.reshape(kv_local, group, 1, 1)
    head_out = final[2] / final[1][..., None] - weight * final[5] / final[4][..., None]
    head_out = head_out * lax.rsqrt(jnp.mean(head_out * head_out, axis=-1, keepdims=True) + 1e-05)
    return (
        head_out.transpose(2, 0, 1, 3)
        .reshape(count, kv_local * group * value_dim)
        .astype(jnp.bfloat16)
    )


def shared_part(normed, s_gate, s_up, s_down):
    piece = lax.all_gather(normed, "tp", axis=0, tiled=True)
    gate_part = jnp.dot(piece, s_gate, preferred_element_type=jnp.float32)
    up_part = jnp.dot(piece, s_up, preferred_element_type=jnp.float32)
    hidden = (jax.nn.silu(gate_part) * up_part).astype(jnp.bfloat16)
    terms = jnp.dot(hidden, s_down, preferred_element_type=jnp.float32)
    return lax.psum_scatter(
        terms.astype(jnp.bfloat16), "tp", scatter_dimension=0, tiled=True
    ).astype(jnp.float32)


def routed_part(normed, routes, route_w, w_gate, w_up, w_down):
    rows, topk = routes.shape
    local_experts = w_gate.shape[0]
    experts = local_experts * lax.axis_size("sp")
    slots = max(2, 3 * rows * topk // (2 * experts))
    flat_ids = routes.reshape(-1)
    hits = (flat_ids[:, None] == jnp.arange(experts, dtype=jnp.int32)[None, :]).astype(jnp.int32)
    slot_of = jnp.sum(jnp.cumsum(hits, axis=0) * hits, axis=1) - 1
    target = flat_ids * slots + slot_of
    placing = jnp.any(
        jnp.arange(experts * slots, dtype=jnp.int32)[:, None, None]
        == target.reshape(rows, topk)[None, :, :],
        axis=-1,
    ).astype(jnp.bfloat16)
    outgoing = (
        jnp.dot(placing, normed, preferred_element_type=jnp.float32)
        .astype(jnp.bfloat16)
        .reshape(experts, slots, normed.shape[1])
    )
    arrived = lax.all_to_all(outgoing, "sp", split_axis=0, concat_axis=0, tiled=True)
    sources = arrived.shape[0] // local_experts
    grouped = arrived.reshape(sources, local_experts, arrived.shape[1], arrived.shape[2])
    gate_part = jnp.einsum("sjcd,jdf->sjcf", grouped, w_gate, preferred_element_type=jnp.float32)
    up_part = jnp.einsum("sjcd,jdf->sjcf", grouped, w_up, preferred_element_type=jnp.float32)
    hidden = (jax.nn.silu(gate_part) * up_part).astype(jnp.bfloat16)
    result = jnp.einsum(
        "sjcf,jfd->sjcd", hidden, w_down, preferred_element_type=jnp.float32
    ).astype(jnp.bfloat16)
    returned = lax.all_to_all(
        result.reshape(arrived.shape), "sp", split_axis=0, concat_axis=0, tiled=True
    )
    picked = (
        returned.reshape(experts * slots, normed.shape[1])[target]
        .reshape(rows, topk, normed.shape[1])
        .astype(jnp.float32)
    )
    return jnp.sum(picked * route_w[..., None], axis=1)


def slow_local(
    stream_in,
    q_first,
    q_second,
    k_first,
    k_second,
    values,
    head_lambda,
    w_out,
    norm_gain,
    routes,
    route_w,
    w_gate,
    w_up,
    w_down,
    s_gate,
    s_up,
    s_down,
):
    seq_rows = q_first.shape[0]
    kv_local = k_first.shape[1] // HEAD
    heads_local = q_first.shape[1] // HEAD
    group = heads_local // kv_local
    value_dim = values.shape[1] // kv_local
    offset = lax.axis_index("sp") * seq_rows
    query_pos = offset + jnp.arange(seq_rows, dtype=jnp.int32)
    last_row = offset + seq_rows - 1
    first_q = q_first.reshape(seq_rows, kv_local, group, HEAD)
    second_q = q_second.reshape(seq_rows, kv_local, group, HEAD)
    start_state = empty_state(kv_local, group, seq_rows, value_dim)
    folded_state = fold_rows(
        start_state,
        first_q,
        second_q,
        query_pos,
        last_row,
        (
            lax.all_gather(k_first, "sp", axis=0, tiled=True),
            lax.all_gather(k_second, "sp", axis=0, tiled=True),
            lax.all_gather(values, "sp", axis=0, tiled=True),
        ),
        jnp.int32(0),
    )
    attn_rows = finish_heads(folded_state, head_lambda)
    attn = lax.psum_scatter(
        jnp.dot(attn_rows, w_out, preferred_element_type=jnp.float32).astype(jnp.bfloat16),
        "tp",
        scatter_dimension=0,
        tiled=True,
    ).astype(jnp.float32)
    resid = (stream_in.astype(jnp.float32) + attn).astype(jnp.bfloat16)
    stream = lax.optimization_barrier(resid).astype(jnp.float32)
    normed = (
        stream * lax.rsqrt(jnp.mean(stream * stream, axis=-1, keepdims=True) + 1e-06) * norm_gain
    ).astype(jnp.bfloat16)
    routed = routed_part(normed, routes, route_w, w_gate, w_up, w_down)
    shared = shared_part(normed, s_gate, s_up, s_down)
    return (stream + routed + shared).astype(jnp.bfloat16)


VMEM = pltpu.MemorySpace.VMEM
MIB = 1024 * 1024
SMEM = pltpu.MemorySpace.SMEM
HBM = pltpu.MemorySpace.HBM


def ring_order(count):
    return list(range(0, count, 2)) + list(range(count - 1, 0, -2))


def ring_pairs(count):
    order = ring_order(count)
    forward = [(order[i], order[(i + 1) % count]) for i in range(count)]
    return forward, [(b, a) for a, b in forward]


def ring_sources(count):
    order = ring_order(count)
    rows = [None] * count
    for place, index in enumerate(order):
        row = [index]
        for step in range(1, count // 2):
            row += [order[(place - step) % count], order[(place + step) % count]]
        row.append(order[(place + count // 2) % count])
        rows[index] = row
    return rows


def dot_nt(a, b):
    return lax.dot_general(a, b, (((1,), (1,)), ((), ())), preferred_element_type=jnp.float32)


def grouped(copies):
    for copy in copies:
        copy.start()
    return copies


def attn_kernel(blocks, first, last, scale, own_rows, *refs):
    refs = list(refs)
    ids_ref = refs.pop(0)
    if last:
        lam_ref = refs.pop(0)
    q_in = [refs.pop(0), refs.pop(0)]
    kv_in = [[refs.pop(0) for _ in range(pieces)] for _, pieces in blocks]
    if not first:
        state_in = [refs.pop(0) for _ in range(3)]
    if last:
        w, stream, own_ref, send_ref, m_ref, l_ref, acc_ref, mixed_ref = refs
        q_refs = q_in
    elif first:
        *q_refs, m_ref, l_ref, acc_ref = refs
    else:
        m_ref, l_ref, acc_ref = refs
        q_refs = q_in
    rows = q_in[0].shape[0]
    heads = q_in[0].shape[1] // HEAD
    me, mine = ids_ref[0], ids_ref[1]
    outs = (m_ref, l_ref, acc_ref)
    if first:
        for index, turn in enumerate(TURNS):
            start = pl.multiple_of((mine ^ turn) * own_rows, own_rows)
            for which in range(2):
                q_refs[which][index * own_rows : (index + 1) * own_rows] = q_in[which][
                    pl.ds(start, own_rows)
                ]

    def columns(kv_refs, start, stop):
        return jnp.concatenate([ref[:, start:stop] for ref in kv_refs], axis=0)

    def fold(kv_refs, diagonal, old_refs=outs):
        keys = sum(ref.shape[0] for ref in kv_refs)
        v = columns(kv_refs, 2 * HEAD, kv_refs[0].shape[1])
        old_m, old_l, old_acc = old_refs
        if diagonal:
            row_at = lax.broadcasted_iota(jnp.int32, (rows, keys), 0)
            key_at = lax.broadcasted_iota(jnp.int32, (rows, keys), 1)
            part = row_at // own_rows
            place = jnp.zeros_like(part)
            for index, turn in enumerate(TURNS):
                place = jnp.where(part == index, mine ^ turn, place)
            allowed = key_at <= place * own_rows + row_at % own_rows
        for head in range(heads):
            for which in range(2):
                pair = 2 * head + which
                q = q_refs[which][:, head * HEAD : (head + 1) * HEAD]
                k = columns(kv_refs, which * HEAD, (which + 1) * HEAD)
                s = dot_nt(q, k)
                if diagonal:
                    s = jnp.where(allowed, s, FLOOR)
                top = jnp.max(s, axis=1, keepdims=True)
                if diagonal:
                    raised = jnp.broadcast_to(top, (rows, 128))
                else:
                    old = old_m[pair]
                    raised = jnp.maximum(old, top)
                wide = jnp.concatenate([raised] * (keys // 128), axis=1)
                p = jnp.exp((s - wide) * scale)
                part_sum = p[:, :128]
                for at in range(128, keys, 128):
                    part_sum = part_sum + p[:, at : at + 128]
                prod = jnp.dot(p.astype(jnp.bfloat16), v, preferred_element_type=jnp.float32)
                m_ref[pair] = raised
                if diagonal:
                    l_ref[pair] = part_sum
                    acc_ref[pair] = prod
                else:
                    fade = jnp.exp((old - raised) * scale)
                    l_ref[pair] = old_l[pair] * fade + part_sum
                    fades = jnp.concatenate([fade] * (prod.shape[1] // 128), axis=1)
                    acc_ref[pair] = old_acc[pair] * fades + prod

    for index, ((place, _), kv_refs) in enumerate(zip(blocks, kv_in)):
        if first and index == 0:
            fold(kv_refs, True)
            continue
        earlier = ids_ref[2 + place] < me
        carry = not first and index == 0

        @pl.when(earlier)
        def _(kv_refs=kv_refs, carry=carry):
            fold(kv_refs, False, state_in if carry else outs)

        if carry:

            @pl.when(jnp.logical_not(earlier))
            def _():
                for into, source in zip(outs, state_in):
                    into[...] = source[...]

    if last:
        for head in range(heads):
            terms = []
            for which in range(2):
                pair = 2 * head + which
                total = jnp.sum(l_ref[pair], axis=1, keepdims=True)
                terms.append(acc_ref[pair] / total)
            mixed = terms[0] - lam_ref[head] * terms[1]
            square = jnp.mean(mixed * mixed, axis=1, keepdims=True)
            mixed = mixed * lax.rsqrt(square + 1e-05)
            width = mixed.shape[1]
            mixed_ref[:, head * width : (head + 1) * width] = mixed.astype(jnp.bfloat16)
        half = rows // 2
        step = math.gcd(w.shape[1], 512)

        def body(at, _):
            cols = pl.ds(pl.multiple_of(at * step, step), step)
            out = jnp.dot(mixed_ref[...], w[:, cols], preferred_element_type=jnp.float32)
            own_ref[:own_rows, cols] = out[:own_rows] + stream[:, cols].astype(jnp.float32)
            own_ref[own_rows:, cols] = out[own_rows:half]
            send_ref[:, cols] = out[half:].astype(jnp.bfloat16)
            return 0

        lax.fori_loop(0, w.shape[1] // step, body, 0)


def specs(space, count):
    return [pl.BlockSpec(memory_space=space)] * count


def attn_call(ids, q_first, q_second, blocks, state, own_rows, lam=None, w_out=None, stream_in=None):
    rows = q_first.shape[0]
    heads = q_first.shape[1] // HEAD
    pieces = [piece for _, block in blocks for piece in block]
    value_dim = pieces[0].shape[1] - 2 * HEAD
    first, last = state is None, w_out is not None
    states = [
        pltpu.VMEM((2 * heads, rows, 128), jnp.float32),
        pltpu.VMEM((2 * heads, rows, 128), jnp.float32),
        pltpu.VMEM((2 * heads, rows, value_dim), jnp.float32),
    ]
    operands = [ids] + ([lam] if last else [])
    smem = len(operands)
    operands += [q_first, q_second, *pieces, *(() if first else state)]
    scratch = []
    if last:
        operands += [w_out, stream_in]
        width = w_out.shape[1]
        out_shape = [
            pltpu.VMEM((rows // 2, width), jnp.float32),
            jax.ShapeDtypeStruct((rows // 2, width), jnp.bfloat16),
        ]
        scratch = [*states, pltpu.VMEM((rows, heads * value_dim), jnp.bfloat16)]
    else:
        out_shape = list(states)
        if first:
            out_shape = [pltpu.VMEM(q_first.shape, q_first.dtype)] * 2 + out_shape
    keys = sum(piece.shape[0] for piece in pieces)
    plan = tuple((place, len(block)) for place, block in blocks)
    body = lambda *refs: attn_kernel(plan, first, last, HEAD**-0.5, own_rows, *refs)
    return pl.pallas_call(
        body,
        out_shape=out_shape,
        in_specs=specs(SMEM, smem) + specs(VMEM, len(operands) - smem),
        out_specs=specs(VMEM, len(out_shape)),
        scratch_shapes=scratch,
        cost_estimate=pl.CostEstimate(
            flops=8 * heads * rows * keys * (HEAD + value_dim),
            bytes_accessed=4 * 1024 * 1024,
            transcendentals=2 * heads * rows * keys,
        ),
        compiler_params=pltpu.CompilerParams(vmem_limit_bytes=(16 if last else 10) * MIB),
    )(*operands)


def pack_kernel(one_ref, two_ref, three_ref, out_ref, sem):
    wide = one_ref.shape[1]
    cuts = ((0, wide), (wide, wide), (2 * wide, three_ref.shape[1]))
    copies = grouped(
        [
            pltpu.make_async_copy(ref, out_ref.at[:, pl.ds(start, size)], sem.at[at])
            for at, (ref, (start, size)) in enumerate(zip((one_ref, two_ref, three_ref), cuts))
        ]
    )
    for copy in copies:
        copy.wait()


def pack_call(one, two, three):
    width = one.shape[1] + two.shape[1] + three.shape[1]
    return pl.pallas_call(
        pack_kernel,
        out_shape=pltpu.VMEM((one.shape[0], width), one.dtype),
        in_specs=specs(HBM, 3),
        out_specs=pl.BlockSpec(memory_space=VMEM),
        scratch_shapes=[pltpu.SemaphoreType.DMA((3,))],
        name="pack",
    )(one, two, three)


def slices_kernel(unit, at_ref, gate_ref, up_ref, down_ref, gate_out, up_out, down_out, gate, up, turned, sem):
    start = pl.multiple_of(at_ref[0] * unit, unit)
    loads = grouped(
        [
            pltpu.make_async_copy(gate_ref, gate, sem.at[0]),
            pltpu.make_async_copy(up_ref, up, sem.at[1]),
            pltpu.make_async_copy(down_ref.at[pl.ds(start, unit)], down_out, sem.at[2]),
        ]
    )
    for load, source, out in ((loads[0], gate, gate_out), (loads[1], up, up_out)):
        load.wait()
        turned[...] = source[...].T
        out[...] = turned[pl.ds(start, unit)]
    loads[2].wait()


def slices_call(mine, gate, up, down, unit):
    width = gate.shape[0]
    return pl.pallas_call(
        lambda *refs: slices_kernel(unit, *refs),
        out_shape=[pltpu.VMEM((unit, width), gate.dtype)] * 3,
        in_specs=specs(SMEM, 1) + specs(HBM, 3),
        out_specs=specs(VMEM, 3),
        scratch_shapes=[
            pltpu.VMEM(gate.shape, gate.dtype),
            pltpu.VMEM(up.shape, gate.dtype),
            pltpu.VMEM((gate.shape[1], width), gate.dtype),
            pltpu.SemaphoreType.DMA((3,)),
        ],
        name="slices",
    )(mine, gate, up, down)


def combine_kernel(routes_ref, weights_ref, out_ref):
    expert = lax.broadcasted_iota(jnp.int32, out_ref.shape, 1)
    total = jnp.zeros(out_ref.shape, jnp.float32)
    for choice in range(routes_ref.shape[1]):
        chosen = jnp.broadcast_to(routes_ref[:, choice : choice + 1], out_ref.shape)
        weight = jnp.broadcast_to(weights_ref[:, choice : choice + 1], out_ref.shape)
        total += jnp.where(expert == chosen, weight, 0.0)
    out_ref[...] = total


def combine_call(routes, weights):
    return pl.pallas_call(
        combine_kernel,
        out_shape=jax.ShapeDtypeStruct((routes.shape[0], 128), jnp.float32),
        in_specs=specs(VMEM, 2),
        out_specs=pl.BlockSpec(memory_space=VMEM),
        compiler_params=pltpu.CompilerParams(vmem_limit_bytes=2 * MIB),
        name="combine",
    )(routes, weights)


def silu(v):
    return v / (1.0 + jnp.exp(-v))


def spread(ids_ref, combine, count, unit):
    expert = lax.broadcasted_iota(jnp.int32, combine.shape, 1)
    columns = []
    for block in range(count):
        picked = jnp.where(expert == ids_ref[2 + block], combine, 0.0)
        column = jnp.sum(picked, axis=1, keepdims=True)
        columns.append(jnp.broadcast_to(column, (combine.shape[0], unit)))
    return jnp.concatenate(columns, axis=1)


def stack_kernel(plan, *refs):
    sem = refs[-1]
    outs = refs[-1 - len(plan) : -1]
    copies = []
    for out, pieces in zip(outs, plan):
        at = 0
        for which, first, rows in pieces:
            copies.append(
                pltpu.make_async_copy(
                    refs[which].at[pl.ds(first, rows)],
                    out.at[pl.ds(at, rows)],
                    sem.at[len(copies)],
                )
            )
            at += rows
    for copy in grouped(copies):
        copy.wait()


def whole(array):
    return (array, 0, array.shape[0])


def stack_call(*groups):
    operands, plan, shapes = [], [], []
    for group in groups:
        pieces = []
        for array, first, rows in group:
            pieces.append((len(operands), first, rows))
            operands.append(array)
        plan.append(tuple(pieces))
        shapes.append((sum(rows for _, _, rows in group), group[0][0].shape[1]))
    return pl.pallas_call(
        lambda *refs: stack_kernel(tuple(plan), *refs),
        out_shape=[pltpu.VMEM(shape, operands[0].dtype) for shape in shapes],
        in_specs=specs(HBM, len(operands)),
        out_specs=specs(VMEM, len(groups)),
        scratch_shapes=[pltpu.SemaphoreType.DMA((len(operands),))],
        cost_estimate=pl.CostEstimate(flops=10**9, bytes_accessed=16 * MIB, transcendentals=0),
        compiler_params=pltpu.CompilerParams(vmem_limit_bytes=2 * MIB),
        name="stack",
    )(*operands)


def hidden_kernel(unit, ids_ref, one_ref, two_ref, near_ref, far_ref, gate_ref, sg_ref, su_ref, *refs):
    *up_refs, out_ref = refs
    x = jnp.concatenate([one_ref[...], two_ref[...]], axis=0)
    gate = dot_nt(x, gate_ref[...])
    up = dot_nt(x, jnp.concatenate([ref[...] for ref in up_refs], axis=0))
    count = gate.shape[1] // unit
    combine = jnp.concatenate([near_ref[...], far_ref[...]], axis=0)
    hidden = silu(gate) * up * spread(ids_ref, combine, count, unit)
    gate = jnp.dot(x, sg_ref[...], preferred_element_type=jnp.float32)
    up = jnp.dot(x, su_ref[...], preferred_element_type=jnp.float32)
    wide = gate.shape[1]
    out_ref[:, :wide] = (silu(gate) * up).astype(jnp.bfloat16)
    out_ref[:, wide:] = hidden.astype(jnp.bfloat16)


def hidden_call(ids, own, other, combine, ups, gate, s_gate, s_up, unit):
    half, width = own.shape
    total = s_gate.shape[1] + gate.shape[0]
    operands = [ids, own, other, *combine, gate, s_gate, s_up, *ups]
    return pl.pallas_call(
        lambda *refs: hidden_kernel(unit, *refs),
        out_shape=pltpu.VMEM((2 * half, total), jnp.bfloat16),
        in_specs=specs(SMEM, 1) + specs(VMEM, len(operands) - 1),
        out_specs=pl.BlockSpec(memory_space=VMEM),
        cost_estimate=pl.CostEstimate(
            flops=2 * 2 * half * width * 2 * total,
            bytes_accessed=12 * MIB,
            transcendentals=2 * half * total,
        ),
        compiler_params=pltpu.CompilerParams(vmem_limit_bytes=12 * MIB),
        name="hidden",
    )(*operands)


def down_kernel(first, hidden_ref, *refs):
    *down_refs, own_ref, send_ref = refs
    half, width = own_ref.shape
    step = math.gcd(width, 512)
    for at in range(0, width, step):
        cols = slice(first + at, first + at + step)
        down = jnp.concatenate([ref[:, cols] for ref in down_refs], axis=0)
        out = jnp.dot(hidden_ref[...], down, preferred_element_type=jnp.float32)
        own_ref[:, at : at + step] = out[:half]
        send_ref[:, at : at + step] = out[half:].astype(jnp.bfloat16)


def down_call(hidden, downs, first, width):
    rows = hidden.shape[0]
    return pl.pallas_call(
        lambda *refs: down_kernel(first, *refs),
        out_shape=[
            pltpu.VMEM((rows // 2, width), jnp.float32),
            jax.ShapeDtypeStruct((rows // 2, width), jnp.bfloat16),
        ],
        in_specs=specs(VMEM, 1 + len(downs)),
        out_specs=specs(VMEM, 2),
        cost_estimate=pl.CostEstimate(
            flops=2 * rows * width * hidden.shape[1], bytes_accessed=8 * MIB, transcendentals=0
        ),
        compiler_params=pltpu.CompilerParams(vmem_limit_bytes=10 * MIB),
    )(hidden, *downs)


def final_kernel(resid_ref, *refs):
    *parts, out_ref = refs
    rows = out_ref.shape[0]
    width = parts[0].shape[1]
    for at in range(len(parts) // 2):
        cols = slice(at * width, (at + 1) * width)
        total = resid_ref[:rows, cols].astype(jnp.float32) + parts[2 * at][:rows]
        out_ref[:, cols] = (total + parts[2 * at + 1][...].astype(jnp.float32)).astype(
            jnp.bfloat16
        )


def final_call(resid, parts, rows):
    operands = [resid] + [array for part in parts for array in part]
    return pl.pallas_call(
        final_kernel,
        out_shape=jax.ShapeDtypeStruct((rows, resid.shape[1]), jnp.bfloat16),
        in_specs=specs(VMEM, len(operands)),
        out_specs=pl.BlockSpec(memory_space=VMEM),
        compiler_params=pltpu.CompilerParams(vmem_limit_bytes=6 * MIB),
        name="final",
    )(*operands)


def norm_rows(resid, gain):
    stream = resid.astype(jnp.float32)
    return (
        stream * lax.rsqrt(jnp.mean(stream * stream, axis=-1, keepdims=True) + 1e-06) * gain
    ).astype(jnp.bfloat16)


def ring_step(ahead, back, pairs):
    ahead = lax.ppermute(ahead, "sp", pairs[0])
    back = lax.ppermute(back, "sp", pairs[1])
    return ahead, back


def ring_gather(block, count):
    pairs = ring_pairs(count)
    out = [block]
    ahead = back = block
    for _ in range(1, count // 2):
        ahead, back = ring_step(ahead, back, pairs)
        out += [ahead, back]
    half = block.shape[0] // 2
    low, high = ring_step(ahead[:half], back[half:], pairs)
    return out, low, high


def swap(rows, pairs):
    return lax.ppermute(rows, "tp", pairs)


def fast_local(
    stream_in,
    q_first,
    q_second,
    k_first,
    k_second,
    values,
    head_lambda,
    w_out,
    norm_gain,
    routes,
    route_w,
    w_gate,
    w_up,
    w_down,
    s_gate,
    s_up,
    s_down,
):
    count = lax.axis_size("sp")
    members = lax.axis_size("tp")
    me = lax.axis_index("sp")
    mine = lax.axis_index("tp")
    seq_rows = q_first.shape[0]
    own_rows = seq_rows // members
    unit = w_gate.shape[2] // members
    cores = [(t, t ^ 1) for t in range(members)]
    sides = [(t, t ^ 2) for t in range(members)]

    sources = jnp.asarray(ring_sources(count), jnp.int32)[me]
    ids = jnp.concatenate([jnp.stack([me, mine]).astype(jnp.int32), sources])
    kv = pack_call(k_first, k_second, values)
    blocks, low, high = ring_gather(kv, count)
    gate, up, down = slices_call(mine[None].astype(jnp.int32), w_gate[0], w_up[0], w_down[0], unit)
    gates, gate_low, gate_high = ring_gather(gate, count)
    ups, up_low, up_high = ring_gather(up, count)
    downs, down_low, down_high = ring_gather(down, count)

    queries = (q_first, q_second)
    state = None
    for step in range(1, count // 2):
        begin, end = (0 if step == 1 else 2 * step - 1), 2 * step + 1
        result = attn_call(
            ids,
            *queries,
            [(place, [blocks[place]]) for place in range(begin, end)],
            state,
            own_rows,
        )
        if step == 1:
            queries = result[:2]
        state = result[-3:]
    own, send = attn_call(
        ids, *queries, [(count - 1, [low, high])], state, own_rows, head_lambda, w_out, stream_in
    )

    combine = combine_call(routes, route_w)
    across = swap(combine, sides)
    paired = jnp.concatenate([combine, across])
    combine = (paired, swap(paired, cores))

    met = swap(send, cores)
    pair = (own + met.astype(jnp.float32)).astype(jnp.bfloat16)
    met = swap(pair, sides)
    gate_all, sg, su = stack_call(
        [whole(block) for block in (*gates, gate_low, gate_high)],
        [whole(s_gate)],
        [whole(s_up)],
    )
    resid = (
        pair.astype(jnp.float32)
        + jnp.concatenate([met[own_rows:], met[:own_rows]]).astype(jnp.float32)
    ).astype(jnp.bfloat16)
    resid = lax.optimization_barrier(resid)
    normed = norm_rows(resid, norm_gain)
    other = swap(normed, cores)
    hidden = hidden_call(
        ids, normed, other, combine, [*ups, up_low, up_high], gate_all, sg, su, unit
    )
    downs = [s_down, *downs, down_low, down_high]
    width = stream_in.shape[1] // 2
    sums = []
    for part in range(2):
        sums.append(down_call(hidden, downs, part * width, width))
    parts = []
    for own, send in sums:
        met = swap(send, cores)
        terms = own + met.astype(jnp.float32)
        met = swap(terms[own_rows:].astype(jnp.bfloat16), sides)
        parts.append((terms, met))
    return final_call(resid, parts, own_rows)


def weights_travel(count, members, seq_rows, k_first, values, w_gate):
    unit = w_gate.shape[2] // members
    gathered = 3 * count * unit * w_gate.shape[1] * 2
    return (
        members == 4
        and count >= 4
        and count % 2 == 0
        and w_gate.shape[0] == 1
        and k_first.shape[1] == HEAD
        and values.shape[1] % 128 == 0
        and w_gate.shape[2] % (32 * members) == 0
        and seq_rows % (32 * members) == 0
        and count == 8
        and w_gate.shape[0] * count <= 128
        and gathered <= 16 * 1024 * 1024
    )


def local(*args):
    count, members = lax.axis_size("sp"), lax.axis_size("tp")
    if weights_travel(count, members, args[1].shape[0], args[3], args[5], args[11]):
        return fast_local(*args)
    return slow_local(*args)


def solution(mesh):
    return jax.shard_map(
        local,
        mesh=mesh,
        in_specs=(
            P(("sp", "tp"), None),
            P("sp", "tp"),
            P("sp", "tp"),
            P("sp", "tp"),
            P("sp", "tp"),
            P("sp", "tp"),
            P("tp"),
            P("tp", None),
            P(),
            P(("sp", "tp"), None),
            P(("sp", "tp"), None),
            P("sp", None, None),
            P("sp", None, None),
            P("sp", None, None),
            P(None, "tp"),
            P(None, "tp"),
            P("tp", None),
        ),
        out_specs=P(("sp", "tp"), None),
        check_vma=False,
    )
```

```python
import math

import jax
import jax.numpy as jnp
from jax import lax
from jax.experimental import pallas as pl
from jax.experimental.pallas import tpu as pltpu
from jax.sharding import PartitionSpec as P

HEAD = 128
TURNS = (0, 2, 1, 3)


FLOOR = -1e30


def absorb(state, first_q, second_q, first_k, second_k, value_rows, query_pos, key_pos):
    allowed = key_pos[None, :] <= query_pos[:, None]
    scale = first_q.shape[-1] ** (-0.5)
    result = []
    pairs = ((first_q, first_k), (second_q, second_k))
    for index in range(2):
        query_rows, key_rows = pairs[index]
        peak, total, accum = (state[3 * index], state[3 * index + 1], state[3 * index + 2])
        scores = (
            jnp.einsum("qagd,kad->agqk", query_rows, key_rows, preferred_element_type=jnp.float32)
            * scale
        )
        scores = jnp.where(allowed, scores, FLOOR)
        raised = jnp.maximum(peak, scores.max(-1))
        weights = jnp.where(allowed, jnp.exp(scores - raised[..., None]), 0.0)
        fade = jnp.exp(peak - raised)
        total = total * fade + weights.sum(-1)
        accum = accum * fade[..., None] + jnp.einsum(
            "agqk,kad->agqd",
            weights.astype(jnp.bfloat16),
            value_rows,
            preferred_element_type=jnp.float32,
        )
        result += [raised, total, accum]
    return tuple(result)


def empty_state(kv_local, group, count, value_dim):
    peaks = jnp.full((kv_local, group, count), FLOOR, jnp.float32)
    sums = jnp.zeros((kv_local, group, count), jnp.float32)
    accums = jnp.zeros((kv_local, group, count, value_dim), jnp.float32)
    return (peaks, sums, accums, peaks, sums, accums)


def fold_rows(state, first_q, second_q, query_pos, last_row, pieces, start):
    first_k, second_k, value_rows = pieces
    length = first_k.shape[0]
    kv_local = first_q.shape[1]
    value_dim = value_rows.shape[1] // kv_local
    span = math.gcd(length, 2048)

    def sweep(current):

        def visit(block, inner):
            begin = block * span
            key_one = lax.dynamic_slice_in_dim(first_k, begin, span, 0).reshape(
                span, kv_local, HEAD
            )
            key_two = lax.dynamic_slice_in_dim(second_k, begin, span, 0).reshape(
                span, kv_local, HEAD
            )
            value_part = lax.dynamic_slice_in_dim(value_rows, begin, span, 0).reshape(
                span, kv_local, value_dim
            )
            key_pos = begin + jnp.arange(span, dtype=jnp.int32)
            return absorb(
                inner, first_q, second_q, key_one, key_two, value_part, query_pos, key_pos
            )

        return lax.fori_loop(0, length // span, visit, current)

    def unchanged(current):
        return current

    return lax.cond(start <= last_row, sweep, unchanged, state)


def finish_heads(final, head_lambda):
    kv_local, group, count, value_dim = final[2].shape
    weight = head_lambda.reshape(kv_local, group, 1, 1)
    head_out = final[2] / final[1][..., None] - weight * final[5] / final[4][..., None]
    head_out = head_out * lax.rsqrt(jnp.mean(head_out * head_out, axis=-1, keepdims=True) + 1e-05)
    return (
        head_out.transpose(2, 0, 1, 3)
        .reshape(count, kv_local * group * value_dim)
        .astype(jnp.bfloat16)
    )


def shared_part(normed, s_gate, s_up, s_down):
    piece = lax.all_gather(normed, "tp", axis=0, tiled=True)
    gate_part = jnp.dot(piece, s_gate, preferred_element_type=jnp.float32)
    up_part = jnp.dot(piece, s_up, preferred_element_type=jnp.float32)
    hidden = (jax.nn.silu(gate_part) * up_part).astype(jnp.bfloat16)
    terms = jnp.dot(hidden, s_down, preferred_element_type=jnp.float32)
    return lax.psum_scatter(
        terms.astype(jnp.bfloat16), "tp", scatter_dimension=0, tiled=True
    ).astype(jnp.float32)


def routed_part(normed, routes, route_w, w_gate, w_up, w_down):
    rows, topk = routes.shape
    local_experts = w_gate.shape[0]
    experts = local_experts * lax.axis_size("sp")
    slots = max(2, 3 * rows * topk // (2 * experts))
    flat_ids = routes.reshape(-1)
    hits = (flat_ids[:, None] == jnp.arange(experts, dtype=jnp.int32)[None, :]).astype(jnp.int32)
    slot_of = jnp.sum(jnp.cumsum(hits, axis=0) * hits, axis=1) - 1
    target = flat_ids * slots + slot_of
    placing = jnp.any(
        jnp.arange(experts * slots, dtype=jnp.int32)[:, None, None]
        == target.reshape(rows, topk)[None, :, :],
        axis=-1,
    ).astype(jnp.bfloat16)
    outgoing = (
        jnp.dot(placing, normed, preferred_element_type=jnp.float32)
        .astype(jnp.bfloat16)
        .reshape(experts, slots, normed.shape[1])
    )
    arrived = lax.all_to_all(outgoing, "sp", split_axis=0, concat_axis=0, tiled=True)
    sources = arrived.shape[0] // local_experts
    grouped = arrived.reshape(sources, local_experts, arrived.shape[1], arrived.shape[2])
    gate_part = jnp.einsum("sjcd,jdf->sjcf", grouped, w_gate, preferred_element_type=jnp.float32)
    up_part = jnp.einsum("sjcd,jdf->sjcf", grouped, w_up, preferred_element_type=jnp.float32)
    hidden = (jax.nn.silu(gate_part) * up_part).astype(jnp.bfloat16)
    result = jnp.einsum(
        "sjcf,jfd->sjcd", hidden, w_down, preferred_element_type=jnp.float32
    ).astype(jnp.bfloat16)
    returned = lax.all_to_all(
        result.reshape(arrived.shape), "sp", split_axis=0, concat_axis=0, tiled=True
    )
    picked = (
        returned.reshape(experts * slots, normed.shape[1])[target]
        .reshape(rows, topk, normed.shape[1])
        .astype(jnp.float32)
    )
    return jnp.sum(picked * route_w[..., None], axis=1)


def slow_local(
    stream_in,
    q_first,
    q_second,
    k_first,
    k_second,
    values,
    head_lambda,
    w_out,
    norm_gain,
    routes,
    route_w,
    w_gate,
    w_up,
    w_down,
    s_gate,
    s_up,
    s_down,
):
    seq_rows = q_first.shape[0]
    kv_local = k_first.shape[1] // HEAD
    heads_local = q_first.shape[1] // HEAD
    group = heads_local // kv_local
    value_dim = values.shape[1] // kv_local
    offset = lax.axis_index("sp") * seq_rows
    query_pos = offset + jnp.arange(seq_rows, dtype=jnp.int32)
    last_row = offset + seq_rows - 1
    first_q = q_first.reshape(seq_rows, kv_local, group, HEAD)
    second_q = q_second.reshape(seq_rows, kv_local, group, HEAD)
    start_state = empty_state(kv_local, group, seq_rows, value_dim)
    folded_state = fold_rows(
        start_state,
        first_q,
        second_q,
        query_pos,
        last_row,
        (
            lax.all_gather(k_first, "sp", axis=0, tiled=True),
            lax.all_gather(k_second, "sp", axis=0, tiled=True),
            lax.all_gather(values, "sp", axis=0, tiled=True),
        ),
        jnp.int32(0),
    )
    attn_rows = finish_heads(folded_state, head_lambda)
    attn = lax.psum_scatter(
        jnp.dot(attn_rows, w_out, preferred_element_type=jnp.float32).astype(jnp.bfloat16),
        "tp",
        scatter_dimension=0,
        tiled=True,
    ).astype(jnp.float32)
    resid = (stream_in.astype(jnp.float32) + attn).astype(jnp.bfloat16)
    stream = lax.optimization_barrier(resid).astype(jnp.float32)
    normed = (
        stream * lax.rsqrt(jnp.mean(stream * stream, axis=-1, keepdims=True) + 1e-06) * norm_gain
    ).astype(jnp.bfloat16)
    routed = routed_part(normed, routes, route_w, w_gate, w_up, w_down)
    shared = shared_part(normed, s_gate, s_up, s_down)
    return (stream + routed + shared).astype(jnp.bfloat16)


VMEM = pltpu.MemorySpace.VMEM
MIB = 1024 * 1024
SMEM = pltpu.MemorySpace.SMEM
HBM = pltpu.MemorySpace.HBM


def ring_order(count):
    return list(range(0, count, 2)) + list(range(count - 1, 0, -2))


def ring_pairs(count):
    order = ring_order(count)
    forward = [(order[i], order[(i + 1) % count]) for i in range(count)]
    return forward, [(b, a) for a, b in forward]


def ring_sources(count):
    order = ring_order(count)
    rows = [None] * count
    for place, index in enumerate(order):
        row = [index]
        for step in range(1, count // 2):
            row += [order[(place - step) % count], order[(place + step) % count]]
        row.append(order[(place + count // 2) % count])
        rows[index] = row
    return rows


def dot_nt(a, b):
    return lax.dot_general(a, b, (((1,), (1,)), ((), ())), preferred_element_type=jnp.float32)


def grouped(copies):
    for copy in copies:
        copy.start()
    return copies


def attn_kernel(blocks, first, last, scale, own_rows, *refs):
    refs = list(refs)
    ids_ref = refs.pop(0)
    if last:
        lam_ref = refs.pop(0)
    q_in = [refs.pop(0), refs.pop(0)]
    kv_in = [[refs.pop(0) for _ in range(pieces)] for _, pieces in blocks]
    if not first:
        state_in = [refs.pop(0) for _ in range(3)]
    if last:
        w, stream, own_ref, send_ref, m_ref, l_ref, acc_ref, mixed_ref = refs
        q_refs = q_in
    elif first:
        *q_refs, m_ref, l_ref, acc_ref = refs
    else:
        m_ref, l_ref, acc_ref = refs
        q_refs = q_in
    rows = q_in[0].shape[0]
    heads = q_in[0].shape[1] // HEAD
    me, mine = ids_ref[0], ids_ref[1]
    outs = (m_ref, l_ref, acc_ref)
    if first:
        for index, turn in enumerate(TURNS):
            start = pl.multiple_of((mine ^ turn) * own_rows, own_rows)
            for which in range(2):
                q_refs[which][index * own_rows : (index + 1) * own_rows] = q_in[which][
                    pl.ds(start, own_rows)
                ]

    def columns(kv_refs, start, stop):
        return jnp.concatenate([ref[:, start:stop] for ref in kv_refs], axis=0)

    def fold(kv_refs, diagonal, old_refs=outs):
        keys = sum(ref.shape[0] for ref in kv_refs)
        v = columns(kv_refs, 2 * HEAD, kv_refs[0].shape[1])
        old_m, old_l, old_acc = old_refs
        if diagonal:
            row_at = lax.broadcasted_iota(jnp.int32, (rows, keys), 0)
            key_at = lax.broadcasted_iota(jnp.int32, (rows, keys), 1)
            part = row_at // own_rows
            place = jnp.zeros_like(part)
            for index, turn in enumerate(TURNS):
                place = jnp.where(part == index, mine ^ turn, place)
            allowed = key_at <= place * own_rows + row_at % own_rows
        for head in range(heads):
            for which in range(2):
                pair = 2 * head + which
                q = q_refs[which][:, head * HEAD : (head + 1) * HEAD]
                k = columns(kv_refs, which * HEAD, (which + 1) * HEAD)
                s = dot_nt(q, k)
                if diagonal:
                    s = jnp.where(allowed, s, FLOOR)
                top = jnp.max(s, axis=1, keepdims=True)
                if diagonal:
                    raised = jnp.broadcast_to(top, (rows, 128))
                else:
                    old = old_m[pair]
                    raised = jnp.maximum(old, top)
                wide = jnp.concatenate([raised] * (keys // 128), axis=1)
                p = jnp.exp((s - wide) * scale)
                part_sum = p[:, :128]
                for at in range(128, keys, 128):
                    part_sum = part_sum + p[:, at : at + 128]
                prod = jnp.dot(p.astype(jnp.bfloat16), v, preferred_element_type=jnp.float32)
                m_ref[pair] = raised
                if diagonal:
                    l_ref[pair] = part_sum
                    acc_ref[pair] = prod
                else:
                    fade = jnp.exp((old - raised) * scale)
                    l_ref[pair] = old_l[pair] * fade + part_sum
                    fades = jnp.concatenate([fade] * (prod.shape[1] // 128), axis=1)
                    acc_ref[pair] = old_acc[pair] * fades + prod

    for index, ((place, _), kv_refs) in enumerate(zip(blocks, kv_in)):
        if first and index == 0:
            fold(kv_refs, True)
            continue
        earlier = ids_ref[2 + place] < me
        carry = not first and index == 0

        @pl.when(earlier)
        def _(kv_refs=kv_refs, carry=carry):
            fold(kv_refs, False, state_in if carry else outs)

        if carry:

            @pl.when(jnp.logical_not(earlier))
            def _():
                for into, source in zip(outs, state_in):
                    into[...] = source[...]

    if last:
        for head in range(heads):
            terms = []
            for which in range(2):
                pair = 2 * head + which
                total = jnp.sum(l_ref[pair], axis=1, keepdims=True)
                terms.append(acc_ref[pair] / total)
            mixed = terms[0] - lam_ref[head] * terms[1]
            square = jnp.mean(mixed * mixed, axis=1, keepdims=True)
            mixed = mixed * lax.rsqrt(square + 1e-05)
            width = mixed.shape[1]
            mixed_ref[:, head * width : (head + 1) * width] = mixed.astype(jnp.bfloat16)
        half = rows // 2
        step = math.gcd(w.shape[1], 512)

        def body(at, _):
            cols = pl.ds(pl.multiple_of(at * step, step), step)
            out = jnp.dot(mixed_ref[...], w[:, cols], preferred_element_type=jnp.float32)
            own_ref[:own_rows, cols] = out[:own_rows] + stream[:, cols].astype(jnp.float32)
            own_ref[own_rows:, cols] = out[own_rows:half]
            send_ref[:, cols] = out[half:].astype(jnp.bfloat16)
            return 0

        lax.fori_loop(0, w.shape[1] // step, body, 0)


def specs(space, count):
    return [pl.BlockSpec(memory_space=space)] * count


def attn_call(ids, q_first, q_second, blocks, state, own_rows, lam=None, w_out=None, stream_in=None):
    rows = q_first.shape[0]
    heads = q_first.shape[1] // HEAD
    pieces = [piece for _, block in blocks for piece in block]
    value_dim = pieces[0].shape[1] - 2 * HEAD
    first, last = state is None, w_out is not None
    states = [
        pltpu.VMEM((2 * heads, rows, 128), jnp.float32),
        pltpu.VMEM((2 * heads, rows, 128), jnp.float32),
        pltpu.VMEM((2 * heads, rows, value_dim), jnp.float32),
    ]
    operands = [ids] + ([lam] if last else [])
    smem = len(operands)
    operands += [q_first, q_second, *pieces, *(() if first else state)]
    scratch = []
    if last:
        operands += [w_out, stream_in]
        width = w_out.shape[1]
        out_shape = [
            pltpu.VMEM((rows // 2, width), jnp.float32),
            jax.ShapeDtypeStruct((rows // 2, width), jnp.bfloat16),
        ]
        scratch = [*states, pltpu.VMEM((rows, heads * value_dim), jnp.bfloat16)]
    else:
        out_shape = list(states)
        if first:
            out_shape = [pltpu.VMEM(q_first.shape, q_first.dtype)] * 2 + out_shape
    keys = sum(piece.shape[0] for piece in pieces)
    plan = tuple((place, len(block)) for place, block in blocks)
    body = lambda *refs: attn_kernel(plan, first, last, HEAD**-0.5, own_rows, *refs)
    return pl.pallas_call(
        body,
        out_shape=out_shape,
        in_specs=specs(SMEM, smem) + specs(VMEM, len(operands) - smem),
        out_specs=specs(VMEM, len(out_shape)),
        scratch_shapes=scratch,
        cost_estimate=pl.CostEstimate(
            flops=8 * heads * rows * keys * (HEAD + value_dim),
            bytes_accessed=4 * 1024 * 1024,
            transcendentals=2 * heads * rows * keys,
        ),
        compiler_params=pltpu.CompilerParams(vmem_limit_bytes=(16 if last else 10) * MIB),
    )(*operands)


def pack_kernel(one_ref, two_ref, three_ref, out_ref, sem):
    wide = one_ref.shape[1]
    cuts = ((0, wide), (wide, wide), (2 * wide, three_ref.shape[1]))
    copies = grouped(
        [
            pltpu.make_async_copy(ref, out_ref.at[:, pl.ds(start, size)], sem.at[at])
            for at, (ref, (start, size)) in enumerate(zip((one_ref, two_ref, three_ref), cuts))
        ]
    )
    for copy in copies:
        copy.wait()


def pack_call(one, two, three):
    width = one.shape[1] + two.shape[1] + three.shape[1]
    return pl.pallas_call(
        pack_kernel,
        out_shape=pltpu.VMEM((one.shape[0], width), one.dtype),
        in_specs=specs(HBM, 3),
        out_specs=pl.BlockSpec(memory_space=VMEM),
        scratch_shapes=[pltpu.SemaphoreType.DMA((3,))],
        name="pack",
    )(one, two, three)


def slices_kernel(unit, at_ref, gate_ref, up_ref, down_ref, gate_out, up_out, down_out, gate, up, turned, sem):
    start = pl.multiple_of(at_ref[0] * unit, unit)
    loads = grouped(
        [
            pltpu.make_async_copy(gate_ref, gate, sem.at[0]),
            pltpu.make_async_copy(up_ref, up, sem.at[1]),
            pltpu.make_async_copy(down_ref.at[pl.ds(start, unit)], down_out, sem.at[2]),
        ]
    )
    for load, source, out in ((loads[0], gate, gate_out), (loads[1], up, up_out)):
        load.wait()
        turned[...] = source[...].T
        out[...] = turned[pl.ds(start, unit)]
    loads[2].wait()


def slices_call(mine, gate, up, down, unit):
    width = gate.shape[0]
    return pl.pallas_call(
        lambda *refs: slices_kernel(unit, *refs),
        out_shape=[pltpu.VMEM((unit, width), gate.dtype)] * 3,
        in_specs=specs(SMEM, 1) + specs(HBM, 3),
        out_specs=specs(VMEM, 3),
        scratch_shapes=[
            pltpu.VMEM(gate.shape, gate.dtype),
            pltpu.VMEM(up.shape, gate.dtype),
            pltpu.VMEM((gate.shape[1], width), gate.dtype),
            pltpu.SemaphoreType.DMA((3,)),
        ],
        name="slices",
    )(mine, gate, up, down)


def combine_kernel(routes_ref, weights_ref, out_ref):
    expert = lax.broadcasted_iota(jnp.int32, out_ref.shape, 1)
    total = jnp.zeros(out_ref.shape, jnp.float32)
    for choice in range(routes_ref.shape[1]):
        chosen = jnp.broadcast_to(routes_ref[:, choice : choice + 1], out_ref.shape)
        weight = jnp.broadcast_to(weights_ref[:, choice : choice + 1], out_ref.shape)
        total += jnp.where(expert == chosen, weight, 0.0)
    out_ref[...] = total


def combine_call(routes, weights):
    return pl.pallas_call(
        combine_kernel,
        out_shape=jax.ShapeDtypeStruct((routes.shape[0], 128), jnp.float32),
        in_specs=specs(VMEM, 2),
        out_specs=pl.BlockSpec(memory_space=VMEM),
        compiler_params=pltpu.CompilerParams(vmem_limit_bytes=2 * MIB),
        name="combine",
    )(routes, weights)


def silu(v):
    return v / (1.0 + jnp.exp(-v))


def spread(ids_ref, combine, count, unit):
    expert = lax.broadcasted_iota(jnp.int32, combine.shape, 1)
    columns = []
    for block in range(count):
        picked = jnp.where(expert == ids_ref[2 + block], combine, 0.0)
        column = jnp.sum(picked, axis=1, keepdims=True)
        columns.append(jnp.broadcast_to(column, (combine.shape[0], unit)))
    return jnp.concatenate(columns, axis=1)


def stack_kernel(plan, *refs):
    sem = refs[-1]
    outs = refs[-1 - len(plan) : -1]
    copies = []
    for out, pieces in zip(outs, plan):
        at = 0
        for which, first, rows in pieces:
            copies.append(
                pltpu.make_async_copy(
                    refs[which].at[pl.ds(first, rows)],
                    out.at[pl.ds(at, rows)],
                    sem.at[len(copies)],
                )
            )
            at += rows
    for copy in grouped(copies):
        copy.wait()


def whole(array):
    return (array, 0, array.shape[0])


def stack_call(*groups):
    operands, plan, shapes = [], [], []
    for group in groups:
        pieces = []
        for array, first, rows in group:
            pieces.append((len(operands), first, rows))
            operands.append(array)
        plan.append(tuple(pieces))
        shapes.append((sum(rows for _, _, rows in group), group[0][0].shape[1]))
    return pl.pallas_call(
        lambda *refs: stack_kernel(tuple(plan), *refs),
        out_shape=[pltpu.VMEM(shape, operands[0].dtype) for shape in shapes],
        in_specs=specs(HBM, len(operands)),
        out_specs=specs(VMEM, len(groups)),
        scratch_shapes=[pltpu.SemaphoreType.DMA((len(operands),))],
        cost_estimate=pl.CostEstimate(flops=10**9, bytes_accessed=16 * MIB, transcendentals=0),
        compiler_params=pltpu.CompilerParams(vmem_limit_bytes=2 * MIB),
        name="stack",
    )(*operands)


def hidden_kernel(unit, ids_ref, one_ref, two_ref, near_ref, far_ref, gate_ref, sg_ref, su_ref, *refs):
    *up_refs, out_ref = refs
    x = jnp.concatenate([one_ref[...], two_ref[...]], axis=0)
    gate = dot_nt(x, gate_ref[...])
    up = dot_nt(x, jnp.concatenate([ref[...] for ref in up_refs], axis=0))
    count = gate.shape[1] // unit
    combine = jnp.concatenate([near_ref[...], far_ref[...]], axis=0)
    hidden = silu(gate) * up * spread(ids_ref, combine, count, unit)
    gate = jnp.dot(x, sg_ref[...], preferred_element_type=jnp.float32)
    up = jnp.dot(x, su_ref[...], preferred_element_type=jnp.float32)
    wide = gate.shape[1]
    out_ref[:, :wide] = (silu(gate) * up).astype(jnp.bfloat16)
    out_ref[:, wide:] = hidden.astype(jnp.bfloat16)


def hidden_call(ids, own, other, combine, ups, gate, s_gate, s_up, unit):
    half, width = own.shape
    total = s_gate.shape[1] + gate.shape[0]
    operands = [ids, own, other, *combine, gate, s_gate, s_up, *ups]
    return pl.pallas_call(
        lambda *refs: hidden_kernel(unit, *refs),
        out_shape=pltpu.VMEM((2 * half, total), jnp.bfloat16),
        in_specs=specs(SMEM, 1) + specs(VMEM, len(operands) - 1),
        out_specs=pl.BlockSpec(memory_space=VMEM),
        cost_estimate=pl.CostEstimate(
            flops=2 * 2 * half * width * 2 * total,
            bytes_accessed=12 * MIB,
            transcendentals=2 * half * total,
        ),
        compiler_params=pltpu.CompilerParams(vmem_limit_bytes=12 * MIB),
        name="hidden",
    )(*operands)


def down_kernel(first, hidden_ref, *refs):
    *down_refs, own_ref, send_ref = refs
    half, width = own_ref.shape
    step = math.gcd(width, 512)
    for at in range(0, width, step):
        cols = slice(first + at, first + at + step)
        down = jnp.concatenate([ref[:, cols] for ref in down_refs], axis=0)
        out = jnp.dot(hidden_ref[...], down, preferred_element_type=jnp.float32)
        own_ref[:, at : at + step] = out[:half]
        send_ref[:, at : at + step] = out[half:].astype(jnp.bfloat16)


def down_call(hidden, downs, first, width):
    rows = hidden.shape[0]
    return pl.pallas_call(
        lambda *refs: down_kernel(first, *refs),
        out_shape=[
            pltpu.VMEM((rows // 2, width), jnp.float32),
            jax.ShapeDtypeStruct((rows // 2, width), jnp.bfloat16),
        ],
        in_specs=specs(VMEM, 1 + len(downs)),
        out_specs=specs(VMEM, 2),
        cost_estimate=pl.CostEstimate(
            flops=2 * rows * width * hidden.shape[1], bytes_accessed=8 * MIB, transcendentals=0
        ),
        compiler_params=pltpu.CompilerParams(vmem_limit_bytes=10 * MIB),
    )(hidden, *downs)


def final_kernel(resid_ref, *refs):
    *parts, out_ref = refs
    rows = out_ref.shape[0]
    width = parts[0].shape[1]
    for at in range(len(parts) // 2):
        cols = slice(at * width, (at + 1) * width)
        total = resid_ref[:rows, cols].astype(jnp.float32) + parts[2 * at][:rows]
        out_ref[:, cols] = (total + parts[2 * at + 1][...].astype(jnp.float32)).astype(
            jnp.bfloat16
        )


def final_call(resid, parts, rows):
    operands = [resid] + [array for part in parts for array in part]
    return pl.pallas_call(
        final_kernel,
        out_shape=jax.ShapeDtypeStruct((rows, resid.shape[1]), jnp.bfloat16),
        in_specs=specs(VMEM, len(operands)),
        out_specs=pl.BlockSpec(memory_space=VMEM),
        compiler_params=pltpu.CompilerParams(vmem_limit_bytes=6 * MIB),
        name="final",
    )(*operands)


def norm_rows(resid, gain):
    stream = resid.astype(jnp.float32)
    return (
        stream * lax.rsqrt(jnp.mean(stream * stream, axis=-1, keepdims=True) + 1e-06) * gain
    ).astype(jnp.bfloat16)


def ring_step(ahead, back, pairs):
    ahead = lax.ppermute(ahead, "sp", pairs[0])
    back = lax.ppermute(back, "sp", pairs[1])
    return ahead, back


def ring_gather(block, count):
    pairs = ring_pairs(count)
    out = [block]
    ahead = back = block
    for _ in range(1, count // 2):
        ahead, back = ring_step(ahead, back, pairs)
        out += [ahead, back]
    half = block.shape[0] // 2
    low, high = ring_step(ahead[:half], back[half:], pairs)
    return out, low, high


def ring_gather_fine(block, count):
    pairs = ring_pairs(count)
    out = [block]
    ahead = back = block
    last = count // 2
    for _ in range(1, last - 1):
        ahead, back = ring_step(ahead, back, pairs)
        out += [ahead, back]
    half = block.shape[0] // 2
    ahead_low, back_high = ring_step(ahead[:half], back[half:], pairs)
    ahead_high, back_low = ring_step(ahead[half:], back[:half], pairs)
    low, high = ring_step(ahead_low, back_high, pairs)
    return out + [ahead_low, ahead_high, back_low, back_high, low, high]


def swap(rows, pairs):
    return lax.ppermute(rows, "tp", pairs)


def fast_local(
    stream_in,
    q_first,
    q_second,
    k_first,
    k_second,
    values,
    head_lambda,
    w_out,
    norm_gain,
    routes,
    route_w,
    w_gate,
    w_up,
    w_down,
    s_gate,
    s_up,
    s_down,
):
    count = lax.axis_size("sp")
    members = lax.axis_size("tp")
    me = lax.axis_index("sp")
    mine = lax.axis_index("tp")
    seq_rows = q_first.shape[0]
    own_rows = seq_rows // members
    unit = w_gate.shape[2] // members
    cores = [(t, t ^ 1) for t in range(members)]
    sides = [(t, t ^ 2) for t in range(members)]

    sources = jnp.asarray(ring_sources(count), jnp.int32)[me]
    ids = jnp.concatenate([jnp.stack([me, mine]).astype(jnp.int32), sources])
    kv = pack_call(k_first, k_second, values)
    blocks, low, high = ring_gather(kv, count)
    gate, up, down = slices_call(mine[None].astype(jnp.int32), w_gate[0], w_up[0], w_down[0], unit)
    gates, gate_low, gate_high = ring_gather(gate, count)
    ups, up_low, up_high = ring_gather(up, count)
    downs = ring_gather_fine(down, count)

    queries = (q_first, q_second)
    state = None
    for step in range(1, count // 2):
        begin, end = (0 if step == 1 else 2 * step - 1), 2 * step + 1
        result = attn_call(
            ids,
            *queries,
            [(place, [blocks[place]]) for place in range(begin, end)],
            state,
            own_rows,
        )
        if step == 1:
            queries = result[:2]
        state = result[-3:]
    own, send = attn_call(
        ids, *queries, [(count - 1, [low, high])], state, own_rows, head_lambda, w_out, stream_in
    )

    combine = combine_call(routes, route_w)
    across = swap(combine, sides)
    paired = jnp.concatenate([combine, across])
    combine = (paired, swap(paired, cores))

    met = swap(send, cores)
    pair = (own + met.astype(jnp.float32)).astype(jnp.bfloat16)
    met = swap(pair, sides)
    gate_all, sg, su = stack_call(
        [whole(block) for block in (*gates, gate_low, gate_high)],
        [whole(s_gate)],
        [whole(s_up)],
    )
    resid = (
        pair.astype(jnp.float32)
        + jnp.concatenate([met[own_rows:], met[:own_rows]]).astype(jnp.float32)
    ).astype(jnp.bfloat16)
    resid = lax.optimization_barrier(resid)
    normed = norm_rows(resid, norm_gain)
    other = swap(normed, cores)
    hidden = hidden_call(
        ids, normed, other, combine, [*ups, up_low, up_high], gate_all, sg, su, unit
    )
    downs = [s_down, *downs]
    width = stream_in.shape[1] // 2
    sums = []
    for part in range(2):
        sums.append(down_call(hidden, downs, part * width, width))
    parts = []
    for own, send in sums:
        met = swap(send, cores)
        terms = own + met.astype(jnp.float32)
        met = swap(terms[own_rows:].astype(jnp.bfloat16), sides)
        parts.append((terms, met))
    return final_call(resid, parts, own_rows)


def weights_travel(count, members, seq_rows, k_first, values, w_gate):
    unit = w_gate.shape[2] // members
    gathered = 3 * count * unit * w_gate.shape[1] * 2
    return (
        members == 4
        and count >= 4
        and count % 2 == 0
        and w_gate.shape[0] == 1
        and k_first.shape[1] == HEAD
        and values.shape[1] % 128 == 0
        and w_gate.shape[2] % (32 * members) == 0
        and seq_rows % (32 * members) == 0
        and count == 8
        and w_gate.shape[0] * count <= 128
        and gathered <= 16 * 1024 * 1024
    )


def local(*args):
    count, members = lax.axis_size("sp"), lax.axis_size("tp")
    if weights_travel(count, members, args[1].shape[0], args[3], args[5], args[11]):
        return fast_local(*args)
    return slow_local(*args)


def solution(mesh):
    return jax.shard_map(
        local,
        mesh=mesh,
        in_specs=(
            P(("sp", "tp"), None),
            P("sp", "tp"),
            P("sp", "tp"),
            P("sp", "tp"),
            P("sp", "tp"),
            P("sp", "tp"),
            P("tp"),
            P("tp", None),
            P(),
            P(("sp", "tp"), None),
            P(("sp", "tp"), None),
            P("sp", None, None),
            P("sp", None, None),
            P("sp", None, None),
            P(None, "tp"),
            P(None, "tp"),
            P("tp", None),
        ),
        out_specs=P(("sp", "tp"), None),
        check_vma=False,
    )
```

```python
import math

import jax
import jax.numpy as jnp
from jax import lax
from jax.experimental import pallas as pl
from jax.experimental.pallas import tpu as pltpu
from jax.sharding import PartitionSpec as P

HEAD = 128
TURNS = (0, 2, 1, 3)


FLOOR = -1e30


def absorb(state, first_q, second_q, first_k, second_k, value_rows, query_pos, key_pos):
    allowed = key_pos[None, :] <= query_pos[:, None]
    scale = first_q.shape[-1] ** (-0.5)
    result = []
    pairs = ((first_q, first_k), (second_q, second_k))
    for index in range(2):
        query_rows, key_rows = pairs[index]
        peak, total, accum = (state[3 * index], state[3 * index + 1], state[3 * index + 2])
        scores = (
            jnp.einsum("qagd,kad->agqk", query_rows, key_rows, preferred_element_type=jnp.float32)
            * scale
        )
        scores = jnp.where(allowed, scores, FLOOR)
        raised = jnp.maximum(peak, scores.max(-1))
        weights = jnp.where(allowed, jnp.exp(scores - raised[..., None]), 0.0)
        fade = jnp.exp(peak - raised)
        total = total * fade + weights.sum(-1)
        accum = accum * fade[..., None] + jnp.einsum(
            "agqk,kad->agqd",
            weights.astype(jnp.bfloat16),
            value_rows,
            preferred_element_type=jnp.float32,
        )
        result += [raised, total, accum]
    return tuple(result)


def empty_state(kv_local, group, count, value_dim):
    peaks = jnp.full((kv_local, group, count), FLOOR, jnp.float32)
    sums = jnp.zeros((kv_local, group, count), jnp.float32)
    accums = jnp.zeros((kv_local, group, count, value_dim), jnp.float32)
    return (peaks, sums, accums, peaks, sums, accums)


def fold_rows(state, first_q, second_q, query_pos, last_row, pieces, start):
    first_k, second_k, value_rows = pieces
    length = first_k.shape[0]
    kv_local = first_q.shape[1]
    value_dim = value_rows.shape[1] // kv_local
    span = math.gcd(length, 2048)

    def sweep(current):

        def visit(block, inner):
            begin = block * span
            key_one = lax.dynamic_slice_in_dim(first_k, begin, span, 0).reshape(
                span, kv_local, HEAD
            )
            key_two = lax.dynamic_slice_in_dim(second_k, begin, span, 0).reshape(
                span, kv_local, HEAD
            )
            value_part = lax.dynamic_slice_in_dim(value_rows, begin, span, 0).reshape(
                span, kv_local, value_dim
            )
            key_pos = begin + jnp.arange(span, dtype=jnp.int32)
            return absorb(
                inner, first_q, second_q, key_one, key_two, value_part, query_pos, key_pos
            )

        return lax.fori_loop(0, length // span, visit, current)

    def unchanged(current):
        return current

    return lax.cond(start <= last_row, sweep, unchanged, state)


def finish_heads(final, head_lambda):
    kv_local, group, count, value_dim = final[2].shape
    weight = head_lambda.reshape(kv_local, group, 1, 1)
    head_out = final[2] / final[1][..., None] - weight * final[5] / final[4][..., None]
    head_out = head_out * lax.rsqrt(jnp.mean(head_out * head_out, axis=-1, keepdims=True) + 1e-05)
    return (
        head_out.transpose(2, 0, 1, 3)
        .reshape(count, kv_local * group * value_dim)
        .astype(jnp.bfloat16)
    )


def shared_part(normed, s_gate, s_up, s_down):
    piece = lax.all_gather(normed, "tp", axis=0, tiled=True)
    gate_part = jnp.dot(piece, s_gate, preferred_element_type=jnp.float32)
    up_part = jnp.dot(piece, s_up, preferred_element_type=jnp.float32)
    hidden = (jax.nn.silu(gate_part) * up_part).astype(jnp.bfloat16)
    terms = jnp.dot(hidden, s_down, preferred_element_type=jnp.float32)
    return lax.psum_scatter(
        terms.astype(jnp.bfloat16), "tp", scatter_dimension=0, tiled=True
    ).astype(jnp.float32)


def routed_part(normed, routes, route_w, w_gate, w_up, w_down):
    rows, topk = routes.shape
    local_experts = w_gate.shape[0]
    experts = local_experts * lax.axis_size("sp")
    slots = max(2, 3 * rows * topk // (2 * experts))
    flat_ids = routes.reshape(-1)
    hits = (flat_ids[:, None] == jnp.arange(experts, dtype=jnp.int32)[None, :]).astype(jnp.int32)
    slot_of = jnp.sum(jnp.cumsum(hits, axis=0) * hits, axis=1) - 1
    target = flat_ids * slots + slot_of
    placing = jnp.any(
        jnp.arange(experts * slots, dtype=jnp.int32)[:, None, None]
        == target.reshape(rows, topk)[None, :, :],
        axis=-1,
    ).astype(jnp.bfloat16)
    outgoing = (
        jnp.dot(placing, normed, preferred_element_type=jnp.float32)
        .astype(jnp.bfloat16)
        .reshape(experts, slots, normed.shape[1])
    )
    arrived = lax.all_to_all(outgoing, "sp", split_axis=0, concat_axis=0, tiled=True)
    sources = arrived.shape[0] // local_experts
    grouped = arrived.reshape(sources, local_experts, arrived.shape[1], arrived.shape[2])
    gate_part = jnp.einsum("sjcd,jdf->sjcf", grouped, w_gate, preferred_element_type=jnp.float32)
    up_part = jnp.einsum("sjcd,jdf->sjcf", grouped, w_up, preferred_element_type=jnp.float32)
    hidden = (jax.nn.silu(gate_part) * up_part).astype(jnp.bfloat16)
    result = jnp.einsum(
        "sjcf,jfd->sjcd", hidden, w_down, preferred_element_type=jnp.float32
    ).astype(jnp.bfloat16)
    returned = lax.all_to_all(
        result.reshape(arrived.shape), "sp", split_axis=0, concat_axis=0, tiled=True
    )
    picked = (
        returned.reshape(experts * slots, normed.shape[1])[target]
        .reshape(rows, topk, normed.shape[1])
        .astype(jnp.float32)
    )
    return jnp.sum(picked * route_w[..., None], axis=1)


def slow_local(
    stream_in,
    q_first,
    q_second,
    k_first,
    k_second,
    values,
    head_lambda,
    w_out,
    norm_gain,
    routes,
    route_w,
    w_gate,
    w_up,
    w_down,
    s_gate,
    s_up,
    s_down,
):
    seq_rows = q_first.shape[0]
    kv_local = k_first.shape[1] // HEAD
    heads_local = q_first.shape[1] // HEAD
    group = heads_local // kv_local
    value_dim = values.shape[1] // kv_local
    offset = lax.axis_index("sp") * seq_rows
    query_pos = offset + jnp.arange(seq_rows, dtype=jnp.int32)
    last_row = offset + seq_rows - 1
    first_q = q_first.reshape(seq_rows, kv_local, group, HEAD)
    second_q = q_second.reshape(seq_rows, kv_local, group, HEAD)
    start_state = empty_state(kv_local, group, seq_rows, value_dim)
    folded_state = fold_rows(
        start_state,
        first_q,
        second_q,
        query_pos,
        last_row,
        (
            lax.all_gather(k_first, "sp", axis=0, tiled=True),
            lax.all_gather(k_second, "sp", axis=0, tiled=True),
            lax.all_gather(values, "sp", axis=0, tiled=True),
        ),
        jnp.int32(0),
    )
    attn_rows = finish_heads(folded_state, head_lambda)
    attn = lax.psum_scatter(
        jnp.dot(attn_rows, w_out, preferred_element_type=jnp.float32).astype(jnp.bfloat16),
        "tp",
        scatter_dimension=0,
        tiled=True,
    ).astype(jnp.float32)
    resid = (stream_in.astype(jnp.float32) + attn).astype(jnp.bfloat16)
    stream = lax.optimization_barrier(resid).astype(jnp.float32)
    normed = (
        stream * lax.rsqrt(jnp.mean(stream * stream, axis=-1, keepdims=True) + 1e-06) * norm_gain
    ).astype(jnp.bfloat16)
    routed = routed_part(normed, routes, route_w, w_gate, w_up, w_down)
    shared = shared_part(normed, s_gate, s_up, s_down)
    return (stream + routed + shared).astype(jnp.bfloat16)


VMEM = pltpu.MemorySpace.VMEM
MIB = 1024 * 1024
SMEM = pltpu.MemorySpace.SMEM
HBM = pltpu.MemorySpace.HBM


def ring_order(count):
    return list(range(0, count, 2)) + list(range(count - 1, 0, -2))


def ring_pairs(count):
    order = ring_order(count)
    forward = [(order[i], order[(i + 1) % count]) for i in range(count)]
    return forward, [(b, a) for a, b in forward]


def ring_sources(count):
    order = ring_order(count)
    rows = [None] * count
    for place, index in enumerate(order):
        row = [index]
        for step in range(1, count // 2):
            row += [order[(place - step) % count], order[(place + step) % count]]
        row.append(order[(place + count // 2) % count])
        rows[index] = row
    return rows


def dot_nt(a, b):
    return lax.dot_general(a, b, (((1,), (1,)), ((), ())), preferred_element_type=jnp.float32)


def grouped(copies):
    for copy in copies:
        copy.start()
    return copies


def attn_kernel(blocks, first, last, scale, own_rows, *refs):
    refs = list(refs)
    ids_ref = refs.pop(0)
    if last:
        lam_ref = refs.pop(0)
    q_in = [refs.pop(0), refs.pop(0)]
    kv_in = [[refs.pop(0) for _ in range(pieces)] for _, pieces in blocks]
    if not first:
        state_in = [refs.pop(0) for _ in range(3)]
    if last:
        w, stream, own_ref, send_ref, m_ref, l_ref, acc_ref, mixed_ref = refs
        q_refs = q_in
    elif first:
        *q_refs, m_ref, l_ref, acc_ref = refs
    else:
        m_ref, l_ref, acc_ref = refs
        q_refs = q_in
    rows = q_in[0].shape[0]
    heads = q_in[0].shape[1] // HEAD
    me, mine = ids_ref[0], ids_ref[1]
    outs = (m_ref, l_ref, acc_ref)
    if first:
        for index, turn in enumerate(TURNS):
            start = pl.multiple_of((mine ^ turn) * own_rows, own_rows)
            for which in range(2):
                q_refs[which][index * own_rows : (index + 1) * own_rows] = q_in[which][
                    pl.ds(start, own_rows)
                ]

    def columns(kv_refs, start, stop):
        return jnp.concatenate([ref[:, start:stop] for ref in kv_refs], axis=0)

    def fold(kv_refs, diagonal, old_refs=outs):
        keys = sum(ref.shape[0] for ref in kv_refs)
        v = columns(kv_refs, 2 * HEAD, kv_refs[0].shape[1])
        old_m, old_l, old_acc = old_refs
        if diagonal:
            row_at = lax.broadcasted_iota(jnp.int32, (rows, keys), 0)
            key_at = lax.broadcasted_iota(jnp.int32, (rows, keys), 1)
            part = row_at // own_rows
            place = jnp.zeros_like(part)
            for index, turn in enumerate(TURNS):
                place = jnp.where(part == index, mine ^ turn, place)
            allowed = key_at <= place * own_rows + row_at % own_rows
        for head in range(heads):
            for which in range(2):
                pair = 2 * head + which
                q = q_refs[which][:, head * HEAD : (head + 1) * HEAD]
                k = columns(kv_refs, which * HEAD, (which + 1) * HEAD)
                s = dot_nt(q, k)
                if diagonal:
                    s = jnp.where(allowed, s, FLOOR)
                top = jnp.max(s, axis=1, keepdims=True)
                if diagonal:
                    raised = jnp.broadcast_to(top, (rows, 128))
                else:
                    old = old_m[pair]
                    raised = jnp.maximum(old, top)
                wide = jnp.concatenate([raised] * (keys // 128), axis=1)
                p = jnp.exp((s - wide) * scale)
                part_sum = p[:, :128]
                for at in range(128, keys, 128):
                    part_sum = part_sum + p[:, at : at + 128]
                prod = jnp.dot(p.astype(jnp.bfloat16), v, preferred_element_type=jnp.float32)
                m_ref[pair] = raised
                if diagonal:
                    l_ref[pair] = part_sum
                    acc_ref[pair] = prod
                else:
                    fade = jnp.exp((old - raised) * scale)
                    l_ref[pair] = old_l[pair] * fade + part_sum
                    fades = jnp.concatenate([fade] * (prod.shape[1] // 128), axis=1)
                    acc_ref[pair] = old_acc[pair] * fades + prod

    for index, ((place, _), kv_refs) in enumerate(zip(blocks, kv_in)):
        if first and index == 0:
            fold(kv_refs, True)
            continue
        earlier = ids_ref[2 + place] < me
        carry = not first and index == 0

        @pl.when(earlier)
        def _(kv_refs=kv_refs, carry=carry):
            fold(kv_refs, False, state_in if carry else outs)

        if carry:

            @pl.when(jnp.logical_not(earlier))
            def _():
                for into, source in zip(outs, state_in):
                    into[...] = source[...]

    if last:
        for head in range(heads):
            terms = []
            for which in range(2):
                pair = 2 * head + which
                total = jnp.sum(l_ref[pair], axis=1, keepdims=True)
                terms.append(acc_ref[pair] / total)
            mixed = terms[0] - lam_ref[head] * terms[1]
            square = jnp.mean(mixed * mixed, axis=1, keepdims=True)
            mixed = mixed * lax.rsqrt(square + 1e-05)
            width = mixed.shape[1]
            mixed_ref[:, head * width : (head + 1) * width] = mixed.astype(jnp.bfloat16)
        half = rows // 2
        step = math.gcd(w.shape[1], 512)

        def body(at, _):
            cols = pl.ds(pl.multiple_of(at * step, step), step)
            out = jnp.dot(mixed_ref[...], w[:, cols], preferred_element_type=jnp.float32)
            own_ref[:own_rows, cols] = out[:own_rows] + stream[:, cols].astype(jnp.float32)
            own_ref[own_rows:, cols] = out[own_rows:half]
            send_ref[:, cols] = out[half:].astype(jnp.bfloat16)
            return 0

        lax.fori_loop(0, w.shape[1] // step, body, 0)


def specs(space, count):
    return [pl.BlockSpec(memory_space=space)] * count


def attn_call(ids, q_first, q_second, blocks, state, own_rows, lam=None, w_out=None, stream_in=None):
    rows = q_first.shape[0]
    heads = q_first.shape[1] // HEAD
    pieces = [piece for _, block in blocks for piece in block]
    value_dim = pieces[0].shape[1] - 2 * HEAD
    first, last = state is None, w_out is not None
    states = [
        pltpu.VMEM((2 * heads, rows, 128), jnp.float32),
        pltpu.VMEM((2 * heads, rows, 128), jnp.float32),
        pltpu.VMEM((2 * heads, rows, value_dim), jnp.float32),
    ]
    operands = [ids] + ([lam] if last else [])
    smem = len(operands)
    operands += [q_first, q_second, *pieces, *(() if first else state)]
    scratch = []
    if last:
        operands += [w_out, stream_in]
        width = w_out.shape[1]
        out_shape = [
            pltpu.VMEM((rows // 2, width), jnp.float32),
            jax.ShapeDtypeStruct((rows // 2, width), jnp.bfloat16),
        ]
        scratch = [*states, pltpu.VMEM((rows, heads * value_dim), jnp.bfloat16)]
    else:
        out_shape = list(states)
        if first:
            out_shape = [pltpu.VMEM(q_first.shape, q_first.dtype)] * 2 + out_shape
    keys = sum(piece.shape[0] for piece in pieces)
    plan = tuple((place, len(block)) for place, block in blocks)
    body = lambda *refs: attn_kernel(plan, first, last, HEAD**-0.5, own_rows, *refs)
    return pl.pallas_call(
        body,
        out_shape=out_shape,
        in_specs=specs(SMEM, smem) + specs(VMEM, len(operands) - smem),
        out_specs=specs(VMEM, len(out_shape)),
        scratch_shapes=scratch,
        cost_estimate=pl.CostEstimate(
            flops=8 * heads * rows * keys * (HEAD + value_dim),
            bytes_accessed=4 * 1024 * 1024,
            transcendentals=2 * heads * rows * keys,
        ),
        compiler_params=pltpu.CompilerParams(vmem_limit_bytes=(16 if last else 10) * MIB),
    )(*operands)


def pack_kernel(one_ref, two_ref, three_ref, out_ref, sem):
    wide = one_ref.shape[1]
    cuts = ((0, wide), (wide, wide), (2 * wide, three_ref.shape[1]))
    copies = grouped(
        [
            pltpu.make_async_copy(ref, out_ref.at[:, pl.ds(start, size)], sem.at[at])
            for at, (ref, (start, size)) in enumerate(zip((one_ref, two_ref, three_ref), cuts))
        ]
    )
    for copy in copies:
        copy.wait()


def pack_call(one, two, three):
    width = one.shape[1] + two.shape[1] + three.shape[1]
    return pl.pallas_call(
        pack_kernel,
        out_shape=pltpu.VMEM((one.shape[0], width), one.dtype),
        in_specs=specs(HBM, 3),
        out_specs=pl.BlockSpec(memory_space=VMEM),
        scratch_shapes=[pltpu.SemaphoreType.DMA((3,))],
        name="pack",
    )(one, two, three)


def slices_kernel(unit, at_ref, gate_ref, up_ref, down_ref, gate_out, up_out, down_out, gate, up, turned, sem):
    start = pl.multiple_of(at_ref[0] * unit, unit)
    loads = grouped(
        [
            pltpu.make_async_copy(gate_ref, gate, sem.at[0]),
            pltpu.make_async_copy(up_ref, up, sem.at[1]),
            pltpu.make_async_copy(down_ref.at[pl.ds(start, unit)], down_out, sem.at[2]),
        ]
    )
    for load, source, out in ((loads[0], gate, gate_out), (loads[1], up, up_out)):
        load.wait()
        turned[...] = source[...].T
        out[...] = turned[pl.ds(start, unit)]
    loads[2].wait()


def slices_call(mine, gate, up, down, unit):
    width = gate.shape[0]
    return pl.pallas_call(
        lambda *refs: slices_kernel(unit, *refs),
        out_shape=[pltpu.VMEM((unit, width), gate.dtype)] * 3,
        in_specs=specs(SMEM, 1) + specs(HBM, 3),
        out_specs=specs(VMEM, 3),
        scratch_shapes=[
            pltpu.VMEM(gate.shape, gate.dtype),
            pltpu.VMEM(up.shape, gate.dtype),
            pltpu.VMEM((gate.shape[1], width), gate.dtype),
            pltpu.SemaphoreType.DMA((3,)),
        ],
        name="slices",
    )(mine, gate, up, down)


def combine_kernel(routes_ref, weights_ref, out_ref):
    expert = lax.broadcasted_iota(jnp.int32, out_ref.shape, 1)
    total = jnp.zeros(out_ref.shape, jnp.float32)
    for choice in range(routes_ref.shape[1]):
        chosen = jnp.broadcast_to(routes_ref[:, choice : choice + 1], out_ref.shape)
        weight = jnp.broadcast_to(weights_ref[:, choice : choice + 1], out_ref.shape)
        total += jnp.where(expert == chosen, weight, 0.0)
    out_ref[...] = total


def combine_call(routes, weights):
    return pl.pallas_call(
        combine_kernel,
        out_shape=jax.ShapeDtypeStruct((routes.shape[0], 128), jnp.float32),
        in_specs=specs(VMEM, 2),
        out_specs=pl.BlockSpec(memory_space=VMEM),
        compiler_params=pltpu.CompilerParams(vmem_limit_bytes=2 * MIB),
        name="combine",
    )(routes, weights)


def silu(v):
    return v / (1.0 + jnp.exp(-v))


def spread(ids_ref, combine, count, unit):
    expert = lax.broadcasted_iota(jnp.int32, combine.shape, 1)
    columns = []
    for block in range(count):
        picked = jnp.where(expert == ids_ref[2 + block], combine, 0.0)
        column = jnp.sum(picked, axis=1, keepdims=True)
        columns.append(jnp.broadcast_to(column, (combine.shape[0], unit)))
    return jnp.concatenate(columns, axis=1)


def stack_kernel(plan, *refs):
    sem = refs[-1]
    outs = refs[-1 - len(plan) : -1]
    copies = []
    for out, pieces in zip(outs, plan):
        at = 0
        for which, first, rows in pieces:
            copies.append(
                pltpu.make_async_copy(
                    refs[which].at[pl.ds(first, rows)],
                    out.at[pl.ds(at, rows)],
                    sem.at[len(copies)],
                )
            )
            at += rows
    for copy in grouped(copies):
        copy.wait()


def whole(array):
    return (array, 0, array.shape[0])


def stack_call(*groups):
    operands, plan, shapes = [], [], []
    for group in groups:
        pieces = []
        for array, first, rows in group:
            pieces.append((len(operands), first, rows))
            operands.append(array)
        plan.append(tuple(pieces))
        shapes.append((sum(rows for _, _, rows in group), group[0][0].shape[1]))
    return pl.pallas_call(
        lambda *refs: stack_kernel(tuple(plan), *refs),
        out_shape=[pltpu.VMEM(shape, operands[0].dtype) for shape in shapes],
        in_specs=specs(HBM, len(operands)),
        out_specs=specs(VMEM, len(groups)),
        scratch_shapes=[pltpu.SemaphoreType.DMA((len(operands),))],
        cost_estimate=pl.CostEstimate(flops=10**9, bytes_accessed=16 * MIB, transcendentals=0),
        compiler_params=pltpu.CompilerParams(vmem_limit_bytes=2 * MIB),
        name="stack",
    )(*operands)


def hidden_kernel(unit, ids_ref, one_ref, two_ref, near_ref, far_ref, gate_ref, sg_ref, su_ref, *refs):
    *up_refs, out_ref = refs
    x = jnp.concatenate([one_ref[...], two_ref[...]], axis=0)
    gate = dot_nt(x, gate_ref[...])
    up = dot_nt(x, jnp.concatenate([ref[...] for ref in up_refs], axis=0))
    count = gate.shape[1] // unit
    combine = jnp.concatenate([near_ref[...], far_ref[...]], axis=0)
    hidden = silu(gate) * up * spread(ids_ref, combine, count, unit)
    gate = jnp.dot(x, sg_ref[...], preferred_element_type=jnp.float32)
    up = jnp.dot(x, su_ref[...], preferred_element_type=jnp.float32)
    wide = gate.shape[1]
    out_ref[:, :wide] = (silu(gate) * up).astype(jnp.bfloat16)
    out_ref[:, wide:] = hidden.astype(jnp.bfloat16)


def hidden_call(ids, own, other, combine, ups, gate, s_gate, s_up, unit):
    half, width = own.shape
    total = s_gate.shape[1] + gate.shape[0]
    operands = [ids, own, other, *combine, gate, s_gate, s_up, *ups]
    return pl.pallas_call(
        lambda *refs: hidden_kernel(unit, *refs),
        out_shape=pltpu.VMEM((2 * half, total), jnp.bfloat16),
        in_specs=specs(SMEM, 1) + specs(VMEM, len(operands) - 1),
        out_specs=pl.BlockSpec(memory_space=VMEM),
        cost_estimate=pl.CostEstimate(
            flops=2 * 2 * half * width * 2 * total,
            bytes_accessed=12 * MIB,
            transcendentals=2 * half * total,
        ),
        compiler_params=pltpu.CompilerParams(vmem_limit_bytes=12 * MIB),
        name="hidden",
    )(*operands)


def down_kernel(first, hidden_ref, *refs):
    *down_refs, own_ref, send_ref = refs
    half, width = own_ref.shape
    step = math.gcd(width, 512)
    for at in range(0, width, step):
        cols = slice(first + at, first + at + step)
        down = jnp.concatenate([ref[:, cols] for ref in down_refs], axis=0)
        out = jnp.dot(hidden_ref[...], down, preferred_element_type=jnp.float32)
        own_ref[:, at : at + step] = out[:half]
        send_ref[:, at : at + step] = out[half:].astype(jnp.bfloat16)


def down_call(hidden, downs, first, width):
    rows = hidden.shape[0]
    return pl.pallas_call(
        lambda *refs: down_kernel(first, *refs),
        out_shape=[
            pltpu.VMEM((rows // 2, width), jnp.float32),
            jax.ShapeDtypeStruct((rows // 2, width), jnp.bfloat16),
        ],
        in_specs=specs(VMEM, 1 + len(downs)),
        out_specs=specs(VMEM, 2),
        cost_estimate=pl.CostEstimate(
            flops=2 * rows * width * hidden.shape[1], bytes_accessed=8 * MIB, transcendentals=0
        ),
        compiler_params=pltpu.CompilerParams(vmem_limit_bytes=10 * MIB),
    )(hidden, *downs)


def final_kernel(resid_ref, *refs):
    *parts, out_ref = refs
    rows = out_ref.shape[0]
    width = parts[0].shape[1]
    for at in range(len(parts) // 2):
        cols = slice(at * width, (at + 1) * width)
        total = resid_ref[:rows, cols].astype(jnp.float32) + parts[2 * at][:rows]
        out_ref[:, cols] = (total + parts[2 * at + 1][...].astype(jnp.float32)).astype(
            jnp.bfloat16
        )


def final_call(resid, parts, rows):
    operands = [resid] + [array for part in parts for array in part]
    return pl.pallas_call(
        final_kernel,
        out_shape=jax.ShapeDtypeStruct((rows, resid.shape[1]), jnp.bfloat16),
        in_specs=specs(VMEM, len(operands)),
        out_specs=pl.BlockSpec(memory_space=VMEM),
        compiler_params=pltpu.CompilerParams(vmem_limit_bytes=6 * MIB),
        name="final",
    )(*operands)


def norm_kernel(pair_ref, met_ref, gain_ref, resid_ref, out_ref):
    rows = resid_ref.shape[0]
    for mine, theirs in ((0, 1), (1, 0)):
        here = slice(mine * rows, (mine + 1) * rows)
        there = slice(theirs * rows, (theirs + 1) * rows)
        total = pair_ref[here].astype(jnp.float32) + met_ref[there].astype(jnp.float32)
        resid = total.astype(jnp.bfloat16)
        if mine == 0:
            resid_ref[...] = resid
        stream = resid.astype(jnp.float32)
        square = jnp.mean(stream * stream, axis=1, keepdims=True)
        out_ref[here] = (stream * lax.rsqrt(square + 1e-06) * gain_ref[...]).astype(jnp.bfloat16)


def norm_call(pair, met, gain):
    rows, width = pair.shape
    return pl.pallas_call(
        norm_kernel,
        out_shape=[
            pltpu.VMEM((rows // 2, width), jnp.bfloat16),
            jax.ShapeDtypeStruct((rows, width), jnp.bfloat16),
        ],
        in_specs=specs(VMEM, 3),
        out_specs=specs(VMEM, 2),
        compiler_params=pltpu.CompilerParams(vmem_limit_bytes=6 * MIB),
        name="norm",
    )(pair, met, gain.reshape(1, width))


def ring_step(ahead, back, pairs):
    ahead = lax.ppermute(ahead, "sp", pairs[0])
    back = lax.ppermute(back, "sp", pairs[1])
    return ahead, back


def ring_gather(block, count):
    pairs = ring_pairs(count)
    out = [block]
    ahead = back = block
    for _ in range(1, count // 2):
        ahead, back = ring_step(ahead, back, pairs)
        out += [ahead, back]
    half = block.shape[0] // 2
    low, high = ring_step(ahead[:half], back[half:], pairs)
    return out, low, high


def ring_gather_fine(block, count):
    pairs = ring_pairs(count)
    out = [block]
    ahead = back = block
    last = count // 2
    for _ in range(1, last - 1):
        ahead, back = ring_step(ahead, back, pairs)
        out += [ahead, back]
    half = block.shape[0] // 2
    ahead_low, back_high = ring_step(ahead[:half], back[half:], pairs)
    ahead_high, back_low = ring_step(ahead[half:], back[:half], pairs)
    low, high = ring_step(ahead_low, back_high, pairs)
    return out + [ahead_low, ahead_high, back_low, back_high, low, high]


def swap(rows, pairs):
    return lax.ppermute(rows, "tp", pairs)


def fast_local(
    stream_in,
    q_first,
    q_second,
    k_first,
    k_second,
    values,
    head_lambda,
    w_out,
    norm_gain,
    routes,
    route_w,
    w_gate,
    w_up,
    w_down,
    s_gate,
    s_up,
    s_down,
):
    count = lax.axis_size("sp")
    members = lax.axis_size("tp")
    me = lax.axis_index("sp")
    mine = lax.axis_index("tp")
    seq_rows = q_first.shape[0]
    own_rows = seq_rows // members
    unit = w_gate.shape[2] // members
    cores = [(t, t ^ 1) for t in range(members)]
    sides = [(t, t ^ 2) for t in range(members)]

    sources = jnp.asarray(ring_sources(count), jnp.int32)[me]
    ids = jnp.concatenate([jnp.stack([me, mine]).astype(jnp.int32), sources])
    kv = pack_call(k_first, k_second, values)
    blocks, low, high = ring_gather(kv, count)
    gate, up, down = slices_call(mine[None].astype(jnp.int32), w_gate[0], w_up[0], w_down[0], unit)
    gates, gate_low, gate_high = ring_gather(gate, count)
    ups, up_low, up_high = ring_gather(up, count)
    downs = ring_gather_fine(down, count)

    queries = (q_first, q_second)
    state = None
    for step in range(1, count // 2):
        begin, end = (0 if step == 1 else 2 * step - 1), 2 * step + 1
        result = attn_call(
            ids,
            *queries,
            [(place, [blocks[place]]) for place in range(begin, end)],
            state,
            own_rows,
        )
        if step == 1:
            queries = result[:2]
        state = result[-3:]
    own, send = attn_call(
        ids, *queries, [(count - 1, [low, high])], state, own_rows, head_lambda, w_out, stream_in
    )

    combine = combine_call(routes, route_w)
    across = swap(combine, sides)
    paired = jnp.concatenate([combine, across])
    combine = (paired, swap(paired, cores))

    met = swap(send, cores)
    pair = (own + met.astype(jnp.float32)).astype(jnp.bfloat16)
    met = swap(pair, sides)
    gate_all, sg, su = stack_call(
        [whole(block) for block in (*gates, gate_low, gate_high)],
        [whole(s_gate)],
        [whole(s_up)],
    )
    resid, normed = norm_call(pair, met, norm_gain)
    other = swap(normed, cores)
    hidden = hidden_call(
        ids, normed, other, combine, [*ups, up_low, up_high], gate_all, sg, su, unit
    )
    downs = [s_down, *downs]
    width = stream_in.shape[1] // 2
    sums = []
    for part in range(2):
        sums.append(down_call(hidden, downs, part * width, width))
    parts = []
    for own, send in sums:
        met = swap(send, cores)
        terms = own + met.astype(jnp.float32)
        met = swap(terms[own_rows:].astype(jnp.bfloat16), sides)
        parts.append((terms, met))
    return final_call(resid, parts, own_rows)


def weights_travel(count, members, seq_rows, k_first, values, w_gate):
    unit = w_gate.shape[2] // members
    gathered = 3 * count * unit * w_gate.shape[1] * 2
    return (
        members == 4
        and count >= 4
        and count % 2 == 0
        and w_gate.shape[0] == 1
        and k_first.shape[1] == HEAD
        and values.shape[1] % 128 == 0
        and w_gate.shape[2] % (32 * members) == 0
        and seq_rows % (32 * members) == 0
        and count == 8
        and w_gate.shape[0] * count <= 128
        and gathered <= 16 * 1024 * 1024
    )


def local(*args):
    count, members = lax.axis_size("sp"), lax.axis_size("tp")
    if weights_travel(count, members, args[1].shape[0], args[3], args[5], args[11]):
        return fast_local(*args)
    return slow_local(*args)


def solution(mesh):
    return jax.shard_map(
        local,
        mesh=mesh,
        in_specs=(
            P(("sp", "tp"), None),
            P("sp", "tp"),
            P("sp", "tp"),
            P("sp", "tp"),
            P("sp", "tp"),
            P("sp", "tp"),
            P("tp"),
            P("tp", None),
            P(),
            P(("sp", "tp"), None),
            P(("sp", "tp"), None),
            P("sp", None, None),
            P("sp", None, None),
            P("sp", None, None),
            P(None, "tp"),
            P(None, "tp"),
            P("tp", None),
        ),
        out_specs=P(("sp", "tp"), None),
        check_vma=False,
    )
```
